32 devices in a mesh: sp: 8 (over z, y), tp: 4 (over x, core).
Axes of the slice: x: 2, y: 2, z: 4, core: 2. Of those that a mesh axis runs over, the one named last changes fastest.
Arguments:
- resid: bfloat16 [12288, 2048], P(('sp', 'tp')), may hold values from -6 to 6
- cond: bfloat16 [2048], P('sp'), may hold values from -6 to 6
- mod_shift: bfloat16 [2048, 2048], P('sp', 'tp'), may hold values from -0.125 to 0.125
- mod_scale: bfloat16 [2048, 2048], P('sp', 'tp'), may hold values from -0.125 to 0.125
- mod_gate: bfloat16 [2048, 2048], P('sp', 'tp'), may hold values from -0.125 to 0.125
- norm_gain: float32 [2048], replicated, may hold values from 0.1 to 1.9
- context: bfloat16 [512, 2048], P('sp'), may hold values from -6 to 6
- w_query: bfloat16 [2048, 2048], P(None, 'tp'), may hold values from -0.125 to 0.125
- w_key: bfloat16 [2048, 2048], P(None, 'tp'), may hold values from -0.125 to 0.125
- w_value: bfloat16 [2048, 2048], P(None, 'tp'), may hold values from -0.125 to 0.125
- query_gain: float32 [128], replicated, may hold values from 0.5 to 6, as said below
- key_gain: float32 [128], replicated, may hold values from 0.5 to 6, as said below
- offset_bias: float32 [16, 15, 31], P('tp'), may hold values from -4 to 4
- context_bias: float32 [16], P('tp'), may hold values from -4.5 to 1
- w_out: bfloat16 [2048, 2048], replicated, may hold values from -0.5 to 0.5
Outputs:
- mixed: bfloat16 [12288, 2048], P(('sp', 'tp'))
The draws below stay inside these ranges and needn't reach their ends.
Inputs may be any that keep to these rules, and one draw needn't show every extreme that they name: `query_gain`: positive gains. `key_gain`: positive gains.
All inputs are finite; a program needn't handle non-finite values.
Results may differ from the reference program's by a relative error of at most 0.0085.
The reference program's roundings to bfloat16 on the way count: a program that leaves them out, or rounds other values in their place, can miss the bound.
Values may be sent and summed in bfloat16 or wider, within the bound.
A program may use at most 128 MiB of HBM per device.

```python
import math
import jax
import jax.numpy as jnp
from jax import lax

D = 2048
HEADS = 16
HEAD_DIM = 128
GRID_W = 64
WIN_ROWS = 8
WIN_COLS = 16
ROWS = 192
TOKENS = 12288
CTX = 512


def draw_query_gain(key, part):
    local = jax.random.fold_in(key, 11)
    values = jax.random.uniform(local, (HEAD_DIM,), jnp.float32, 0.6, 1.4)
    return values


def draw_key_gain(key, part):
    local = jax.random.fold_in(key, 23)
    values = jax.random.uniform(local, (HEAD_DIM,), jnp.float32, 0.6, 1.4)
    return values


def draw_context_bias(key, part):
    local = jax.random.fold_in(key, 37)
    level = math.log(float(WIN_ROWS * WIN_COLS) / float(CTX))
    values = jax.random.uniform(local, (HEADS,), jnp.float32, -2.0, -0.5)
    return values + level


def levels(rng, dims, cuts, smallest, high):
    loudness, own = 1.0, jax.random.fold_in(rng, 6)
    for position, shards_of in cuts:
        draws = jnp.exp(jax.random.uniform(jax.random.fold_in(own, position), (shards_of,), jnp.float32, smallest / len(cuts), high / len(cuts)))
        loudness = loudness * jnp.repeat(draws, dims[position] // shards_of).reshape([-1 if axis == position else 1 for axis in range(len(dims))])
    return loudness


def scatter_about(key, extent, scale, most, cuts=(), kind=jnp.bfloat16):
    drawn = scale * jax.random.normal(key, extent, jnp.float32)
    if cuts:
        drawn = drawn * levels(key, extent, cuts, -0.22, 0.18)
    return jnp.clip(drawn, -most, most).astype(kind)


def setup_inputs(seed: int = 0) -> dict:
    streams_of = jax.random.split(jax.random.key(seed), 16)
    return {
        "resid": scatter_about(streams_of[0], (TOKENS, D), 1.0, 6.0, ((0, 32),)),
        "cond": scatter_about(streams_of[1], (D,), 1.0, 6.0, ((0, 8),)),
        "mod_shift": scatter_about(streams_of[2], (D, D), D ** -0.5, 0.125, ((0, 8), (1, 4))),
        "mod_scale": scatter_about(streams_of[3], (D, D), D ** -0.5, 0.125, ((0, 8), (1, 4))),
        "mod_gate": scatter_about(streams_of[4], (D, D), D ** -0.5, 0.125, ((0, 8), (1, 4))),
        "norm_gain": jnp.clip(1.0 + 0.18 * jax.random.normal(streams_of[5], (D,), jnp.float32), 0.1, 1.9),
        "context": scatter_about(streams_of[6], (CTX, D), 1.0, 6.0, ((0, 8),)),
        "w_query": scatter_about(streams_of[7], (D, HEADS * HEAD_DIM), D ** -0.5, 0.125, ((1, 4),)),
        "w_key": scatter_about(streams_of[8], (D, HEADS * HEAD_DIM), D ** -0.5, 0.125, ((1, 4),)),
        "w_value": scatter_about(streams_of[9], (D, HEADS * HEAD_DIM), D ** -0.5, 0.125, ((1, 4),)),
        "query_gain": draw_query_gain(jax.random.fold_in(streams_of[15], 71), 0),
        "key_gain": draw_key_gain(jax.random.fold_in(streams_of[15], 71), 0),
        "offset_bias": scatter_about(streams_of[12], (HEADS, 2 * WIN_ROWS - 1, 2 * WIN_COLS - 1), 1.0, 4.0, ((0, 4),), jnp.float32),
        "context_bias": draw_context_bias(jax.random.fold_in(streams_of[15], 71), 0),
        "w_out": scatter_about(streams_of[14], (HEADS * HEAD_DIM, D), (HEADS * HEAD_DIM // 16) ** -0.5, 0.5),
    }


EPS = 1e-06

def widen(values):
    return lax.optimization_barrier(values).astype(jnp.float32)

def normed_heads(values, gain):
    count = values.shape[0]
    split = values.reshape(count, HEADS, HEAD_DIM)
    scaled = split * lax.rsqrt(lax.optimization_barrier(jnp.mean(split * split, axis=-1, keepdims=True)) + EPS) * gain.astype(jnp.float32)
    return scaled.reshape(count, HEADS * HEAD_DIM).astype(jnp.bfloat16)

def reference(resid, cond, mod_shift, mod_scale, mod_gate, norm_gain, context, w_query, w_key, w_value, query_gain, key_gain, offset_bias, context_bias, w_out):
    lifted = jax.nn.silu(cond.astype(jnp.float32)).astype(jnp.bfloat16)
    shift = jnp.dot(lifted, mod_shift, preferred_element_type=jnp.float32)
    scale = jnp.dot(lifted, mod_scale, preferred_element_type=jnp.float32)
    gate = jnp.dot(lifted, mod_gate, preferred_element_type=jnp.float32)
    floats = resid.astype(jnp.float32)
    inverse = lax.rsqrt(lax.optimization_barrier(jnp.mean(floats * floats, axis=-1, keepdims=True)) + EPS)
    normed = (floats * inverse * norm_gain.astype(jnp.float32) * (1.0 + scale) + shift).astype(jnp.bfloat16)
    query = normed_heads(jnp.dot(normed, w_query, preferred_element_type=jnp.float32), query_gain)
    key = normed_heads(jnp.dot(normed, w_key, preferred_element_type=jnp.float32), key_gain)
    value = jnp.dot(normed, w_value, preferred_element_type=jnp.float32).astype(jnp.bfloat16)
    ctx_floats = context.astype(jnp.float32)
    ctx_inverse = lax.rsqrt(lax.optimization_barrier(jnp.mean(ctx_floats * ctx_floats, axis=-1, keepdims=True)) + EPS)
    ctx_normed = (ctx_floats * ctx_inverse * norm_gain.astype(jnp.float32)).astype(jnp.bfloat16)
    ctx_key = normed_heads(jnp.dot(ctx_normed, w_key, preferred_element_type=jnp.float32), key_gain)
    ctx_value = jnp.dot(ctx_normed, w_value, preferred_element_type=jnp.float32).astype(jnp.bfloat16)
    ctx_key = widen(ctx_key).reshape(CTX, HEADS, HEAD_DIM)
    ctx_value = widen(ctx_value).reshape(CTX, HEADS, HEAD_DIM)
    q_grid = widen(query).reshape(ROWS, GRID_W, HEADS, HEAD_DIM)
    k_grid = widen(key).reshape(ROWS, GRID_W, HEADS, HEAD_DIM)
    v_grid = widen(value).reshape(ROWS, GRID_W, HEADS, HEAD_DIM)
    columns = jnp.arange(GRID_W, dtype=jnp.int32)
    col_start = jnp.clip(columns - WIN_COLS // 2, 0, GRID_W - WIN_COLS)
    valid = (columns[None, :] >= col_start[:, None]) & (columns[None, :] < col_start[:, None] + WIN_COLS)
    col_offset = jnp.clip(columns[None, :] - columns[:, None] + WIN_COLS - 1, 0, 2 * WIN_COLS - 2)
    bias_table = offset_bias.astype(jnp.float32)
    ctx_shift = context_bias.astype(jnp.float32)[:, None, None]
    factor = HEAD_DIM ** (-0.5)

    def one_row(row):
        start = jnp.clip(row - WIN_ROWS // 2, 0, ROWS - WIN_ROWS).astype(jnp.int32)
        queries = lax.dynamic_index_in_dim(q_grid, row, 0, keepdims=False)
        keys = lax.dynamic_slice_in_dim(k_grid, start, WIN_ROWS, 0)
        values = lax.dynamic_slice_in_dim(v_grid, start, WIN_ROWS, 0)
        row_offset = (start + jnp.arange(WIN_ROWS, dtype=jnp.int32) - row + WIN_ROWS - 1).astype(jnp.int32)
        bias = bias_table[:, row_offset][:, :, col_offset]
        s_win = jnp.einsum('qhd,rkhd->hqrk', queries, keys) * factor + jnp.transpose(bias, (0, 2, 1, 3))
        s_win = jnp.where(valid[None, :, None, :], s_win, -1e+30).reshape(HEADS, GRID_W, WIN_ROWS * GRID_W)
        s_ctx = jnp.einsum('qhd,chd->hqc', queries, ctx_key) * factor + ctx_shift
        probs = jax.nn.softmax(jnp.concatenate([s_win, s_ctx], axis=-1), axis=-1).astype(jnp.bfloat16)
        probs = widen(probs)
        p_win = probs[:, :, :WIN_ROWS * GRID_W].reshape(HEADS, GRID_W, WIN_ROWS, GRID_W)
        p_ctx = probs[:, :, WIN_ROWS * GRID_W:]
        out = jnp.einsum('hqrk,rkhd->qhd', p_win, values) + jnp.einsum('hqc,chd->qhd', p_ctx, ctx_value)
        return out.astype(jnp.bfloat16).reshape(GRID_W, HEADS * HEAD_DIM)
    attended = lax.map(one_row, jnp.arange(ROWS, dtype=jnp.int32)).reshape(TOKENS, HEADS * HEAD_DIM)
    projected = jnp.dot(attended, w_out, preferred_element_type=jnp.float32)
    return (floats + gate * projected).astype(jnp.bfloat16)
```

```python
import functools

import jax
import jax.numpy as jnp
from jax import lax
from jax.experimental import pallas as pl
from jax.experimental.pallas import tpu as pltpu
from jax.sharding import PartitionSpec as P

HEAD_DIM = 128
GRID_W = 64
WIN_ROWS = 8
WIN_COLS = 16
REACH = WIN_ROWS // 2
EPS = 1e-06
LOG2E = 1.4426950408889634
MASKED = -1e30
VMEM_BYTES = 60 * 1024 * 1024


def dot32(a, b):
    return jnp.dot(a, b, preferred_element_type=jnp.float32)


def dot_t(a, b):
    return lax.dot_general(a, b, (((1,), (1,)), ((), ())), preferred_element_type=jnp.float32)


def divisor(count, most):
    return max(d for d in range(1, most + 1) if count % d == 0)


def normed_tokens(rows, gain):
    floats = rows.astype(jnp.float32)
    inverse = lax.rsqrt(jnp.mean(floats * floats, axis=-1, keepdims=True) + EPS)
    return floats * inverse * gain


def store_heads(out_ref, at, values, gain):
    count = values.shape[0]
    for h in range(values.shape[1] // HEAD_DIM):
        part = values[:, h * HEAD_DIM : (h + 1) * HEAD_DIM]
        part = part * lax.rsqrt(jnp.mean(part * part, axis=-1, keepdims=True) + EPS) * gain
        out_ref[pl.ds(at, count), h * HEAD_DIM : (h + 1) * HEAD_DIM] = part.astype(jnp.bfloat16)


def fill_bias(ob_ref, table, h):
    rows = 2 * WIN_ROWS - 1
    lanes = 2 * GRID_W
    lane = lax.broadcasted_iota(jnp.int32, (lanes, lanes), 1)
    line = lax.broadcasted_iota(jnp.int32, (lanes, lanes), 0)
    query = line % GRID_W
    begin = jnp.clip(query - WIN_COLS // 2, 0, GRID_W - WIN_COLS)
    valid = (lane >= begin) & (lane < begin + WIN_COLS)

    def spread(r):
        row = jnp.broadcast_to(ob_ref[r, pl.ds(h, 1), :], (GRID_W, lanes))
        return pltpu.roll(row, lanes - (WIN_COLS - 1), 1, stride=1, stride_axis=0)

    masked = jnp.full((GRID_W, lanes), MASKED, jnp.float32)

    def put(slot, first, second):
        both = jnp.concatenate([first, second], axis=0) * LOG2E
        both = jnp.where(valid, both, MASKED)
        table[h, slot] = both.T[:GRID_W]

    low, high = REACH - 1, REACH - 1 + WIN_ROWS
    spreads = [spread(r) for r in range(rows)]
    for r in range(rows + 1):
        put(r, spreads[r] if r < rows else masked, spreads[r - 1] if r > 0 else masked)
    put(rows + 1, spreads[low], masked)
    put(rows + 2, masked, spreads[high - 1])
    table[h, rows + 3] = masked


def layer_kernel(
    sp, tp, chunks, cb_ref, resid, cond, mshift, mscale, mgate, gain_ref, context, wq_hbm, wk_hbm,
    wv_hbm, qg, kg, ob_in, wo_hbm, out_ref,
    tok, wq, wk, wv, wo, qbuf, kvbuf, ctxbuf, ob_ref, table, modsp, modtp, mods, att, full,
    vt, ctxvt, score, prob,
    load_sem, tok_send, pair_send, fwd_send, tok_recv, msp_send, msp_recv, mtp_send, mtp_recv,
    ctx_send, ctx_recv, halo_send, halo_recv, att_send, att_recv,
):
    me_s, me_t = lax.axis_index("sp"), lax.axis_index("tp")
    count, d = resid.shape
    chunk = count // chunks
    width = wq.shape[1]
    heads = width // HEAD_DIM
    tokens = count * tp
    rows = tokens // GRID_W
    total_rows = rows * sp
    first = me_s * rows
    chips = tp // 2
    chip, core = me_t // 2, me_t % 2
    pair = chip * 2 + (1 - core)

    def remote(src, dst, send, recv, axis, peer):
        return pltpu.make_async_remote_copy(
            src_ref=src, dst_ref=dst, send_sem=send, recv_sem=recv,
            device_id={axis: peer}, device_id_type=pl.DeviceIdType.MESH,
        )

    loads = [
        pltpu.make_async_copy(a, b, load_sem.at[i])
        for i, (a, b) in enumerate(
            ((wk_hbm, wk), (wv_hbm, wv), (wq_hbm, wq), (wo_hbm, wo), (resid, tok.at[me_t]))
        )
    ]
    for copy in (loads[4], loads[0], loads[1], loads[2]):
        copy.start()

    barrier = pltpu.get_barrier_semaphore()
    for k in range(1, sp):
        pl.semaphore_signal(
            barrier, inc=1, device_id={"sp": lax.rem(me_s + k, sp)},
            device_id_type=pl.DeviceIdType.MESH,
        )
    for k in range(1, tp):
        pl.semaphore_signal(
            barrier, inc=1, device_id={"tp": lax.rem(me_t + k, tp)},
            device_id_type=pl.DeviceIdType.MESH,
        )
    pl.semaphore_wait(barrier, sp + tp - 2)

    def part(block, c):
        return tok.at[block, pl.ds(pl.multiple_of(c * chunk, chunk), chunk), :]

    def mine(c):
        return resid.at[pl.ds(pl.multiple_of(c * chunk, chunk), chunk), :]

    def across(k, c):
        peer = lax.rem(chip + k, chips) * 2 + core
        return remote(
            mine(c), part(me_t, c), tok_send.at[(k - 1) * chunks + c],
            tok_recv.at[me_t * chunks + c], "tp", peer,
        )

    def beside(c):
        return remote(
            mine(c), part(me_t, c), pair_send.at[c], tok_recv.at[me_t * chunks + c], "tp", pair
        )

    def onward(k, c):
        block = lax.rem(chip + k, chips) * 2 + core
        return remote(
            part(block, c), part(block, c), fwd_send.at[(k - 1) * chunks + c],
            tok_recv.at[block * chunks + c], "tp", pair,
        )

    def arrived(block, c):
        remote(
            part(block, c), part(block, c), pair_send.at[0], tok_recv.at[block * chunks + c],
            "tp", pair,
        ).wait_recv()

    def order(i, side):
        return i + side * (chunks - 1 - 2 * i)

    def across_part(k, c, begin, size):
        peer = lax.rem(chip + k, chips) * 2 + core
        at = pl.ds(pl.multiple_of(c * chunk + begin, 16), size)
        return remote(
            resid.at[at, :], tok.at[me_t, at, :], tok_send.at[(k - 1) * chunks + c],
            tok_recv.at[me_t * chunks + c], "tp", peer,
        )

    early = chunk // 4
    first_chunk = order(0, core)
    for k in range(1, chips):
        across_part(k, first_chunk, 0, early).start()
    for c in range(chunks):
        beside(c).start()

    lifted = cond[...].astype(jnp.float32)
    lifted = (lifted / (1.0 + jnp.exp(-lifted))).astype(jnp.bfloat16)
    lanes = lifted.shape[1]
    for i, m in enumerate((mshift, mscale, mgate)):
        sums = []
        for r in range(lifted.shape[0]):
            line = jnp.broadcast_to(lifted[r : r + 1, :], (16, lanes))
            sums.append(dot32(line, m[r * lanes : (r + 1) * lanes, :])[0:1])
        modsp[me_s, i : i + 1, :] = functools.reduce(jnp.add, sums)
    modsp[me_s, 3:8, :] = jnp.zeros((5, modsp.shape[2]), jnp.float32)

    def to_sp(k, buf, send, recv):
        return remote(
            buf.at[me_s], buf.at[me_s], send.at[k - 1], recv.at[me_s], "sp", lax.rem(me_s + k, sp)
        )

    def from_sp(k, buf, send, recv):
        peer = lax.rem(me_s + k, sp)
        remote(buf.at[peer], buf.at[peer], send.at[k - 1], recv.at[peer], "sp", peer).wait_recv()

    for k in range(1, sp):
        to_sp(k, modsp, msp_send, msp_recv).start()

    loads[0].wait()
    loads[1].wait()
    normed = normed_tokens(context[...], gain_ref[...]).astype(jnp.bfloat16)
    own = ctxbuf.at[me_s]
    store_heads(own, 0, dot32(normed, wk[...]), kg[...])
    own[:, width:] = dot32(normed, wv[...]).astype(jnp.bfloat16)

    for k in range(1, sp):
        from_sp(k, modsp, msp_send, msp_recv)
    summed = modsp[0]
    for s in range(1, sp):
        summed = summed + modsp[s]
    modtp[me_t] = summed

    def to_tp(k):
        return remote(
            modtp.at[me_t], modtp.at[me_t], mtp_send.at[k - 1], mtp_recv.at[me_t], "tp",
            lax.rem(me_t + k, tp),
        )

    for k in range(1, tp):
        to_tp(k).start()
    for k in range(1, chips):
        across_part(k, first_chunk, early, chunk - early).start()
    for i in range(1, chunks):
        for k in range(1, chips):
            across(k, order(i, core)).start()
    for k in range(1, sp):
        to_sp(k, ctxbuf, ctx_send, ctx_recv).start()

    ob_ref[...] = jnp.zeros_like(ob_ref)
    ob_ref[:, :, : ob_in.shape[2]] = ob_in[...]

    def fill(h, carry):
        fill_bias(ob_ref, table, h)
        return carry

    lax.fori_loop(0, heads, fill, 0)

    loads[3].start()
    loads[2].wait()
    loads[4].wait()
    for k in range(1, tp):
        peer = lax.rem(me_t + k, tp)
        remote(
            modtp.at[peer], modtp.at[peer], mtp_send.at[k - 1], mtp_recv.at[peer], "tp", peer
        ).wait_recv()
    piece = modtp.shape[2]
    for t in range(tp):
        mods[:, t * piece : (t + 1) * piece] = modtp[t]

    edge = REACH * GRID_W

    def project(block, c):
        values = tok[block, pl.ds(pl.multiple_of(c * chunk, chunk), chunk), :]
        normed = normed_tokens(values, gain_ref[...]) * (1.0 + mods[1:2, :]) + mods[0:1, :]
        normed = normed.astype(jnp.bfloat16)
        at = pl.multiple_of(block * count + c * chunk, chunk)
        store_heads(qbuf, at, dot32(normed, wq[...]), qg[...])
        at = pl.multiple_of(edge + block * count + c * chunk, GRID_W)
        store_heads(kvbuf, at, dot32(normed, wk[...]), kg[...])
        kvbuf[pl.ds(at, chunk), width:] = dot32(normed, wv[...]).astype(jnp.bfloat16)

    def local_step(c, carry):
        project(me_t, c)
        return carry

    lax.fori_loop(0, chunks, local_step, 0)

    def pair_step(c, carry):
        arrived(pair, c)
        project(pair, c)
        return carry

    lax.fori_loop(0, chunks, pair_step, 0)

    def up():
        return remote(
            kvbuf.at[pl.ds(edge, edge), :], kvbuf.at[pl.ds(edge + tokens, edge), :],
            halo_send.at[0], halo_recv.at[0], "sp", me_s - 1,
        )

    def down():
        return remote(
            kvbuf.at[pl.ds(tokens, edge), :], kvbuf.at[pl.ds(0, edge), :],
            halo_send.at[1], halo_recv.at[1], "sp", me_s + 1,
        )

    upper = chip < (chips + 1) // 2
    lower = jnp.logical_not(upper)

    def send_up(when):
        @pl.when(when & (me_s > 0))
        def _():
            up().start()

    def send_down(when):
        @pl.when(when & (me_s < sp - 1))
        def _():
            down().start()

    @pl.when(me_s == 0)
    def _():
        kvbuf[0:edge, :] = jnp.zeros((edge, 2 * width), jnp.bfloat16)

    @pl.when(me_s == sp - 1)
    def _():
        kvbuf[edge + tokens :, :] = jnp.zeros((edge, 2 * width), jnp.bfloat16)

    ctx_count = ctxbuf.shape[0] * ctxbuf.shape[1]
    factor = HEAD_DIM ** (-0.5) * LOG2E
    span = edge
    blocks = rows // REACH
    half = 2 * GRID_W
    keys = 3 * span
    chunk_rows = rows // tp
    piece_rows = divisor(chunk_rows, 2) if REACH % 2 == 0 else 1
    piece = piece_rows * GRID_W
    per_dest = chunk_rows // piece_rows
    per_block = REACH // piece_rows
    bias_rows = 2 * WIN_ROWS - 1
    plain = list(range(bias_rows + 1))
    lead, trail, blank = bias_rows + 1, bias_rows + 2, bias_rows + 3

    def prepare(kb):
        at = pl.ds(pl.multiple_of(kb * span, span), span)
        vt[:, at] = kvbuf[at, width:].T

    def prepare_context():
        values = ctxbuf[:, :, width:].reshape(ctx_count, width)
        ctxvt[...] = values.T

    def tile_slot(line, side, first, last):
        r = line + REACH - 1 - 2 * side
        low, high = REACH - 1, REACH - 1 + WIN_ROWS
        inner = lead if r == low else trail if r == high else r if low < r < high else blank
        at_first = r if line >= REACH else blank
        at_last = r if line < 2 * REACH else blank
        if inner == at_first == at_last:
            return inner
        return inner + first * (at_first - inner) + last * (at_last - inner)

    def attend(b, first, last):
        at = pl.multiple_of(b * span, span)
        heads = width // HEAD_DIM

        def lanes_of(h, base):
            return slice(base + h * HEAD_DIM, base + (h + 1) * HEAD_DIM)

        def scores(h):
            queries = qbuf[pl.ds(at, span), lanes_of(h, 0)]
            slot = h % 2
            tops = [jnp.full((8, half), MASKED, jnp.float32) for _ in range(2)]
            for kb in range(3):
                part = dot_t(kvbuf[pl.ds(at + kb * span, span), lanes_of(h, 0)], queries)
                for i in range(REACH):
                    line = kb * REACH + i
                    for side in range(2):
                        spot = tile_slot(line, side, first, last)
                        if isinstance(spot, int) and spot == blank:
                            continue
                        cell = part[i * GRID_W : (i + 1) * GRID_W, side * half : (side + 1) * half]
                        cell = cell * factor + table[h, spot]
                        score[slot, line * GRID_W : (line + 1) * GRID_W, side * half : (side + 1) * half] = cell
                        tops[side] = jnp.maximum(tops[side], jnp.max(cell.reshape(-1, 8, half), axis=0))
            raw = jnp.full((8, 2 * half), -jnp.inf, jnp.float32)
            for c in range(ctx_count // span):
                ctx_key = ctxbuf[c * span // ctxbuf.shape[1] : (c + 1) * span // ctxbuf.shape[1], :, lanes_of(h, 0)]
                part = dot_t(ctx_key.reshape(span, HEAD_DIM), queries)
                score[slot, keys + c * span : keys + (c + 1) * span, :] = part
                raw = jnp.maximum(raw, jnp.max(part.reshape(-1, 8, 2 * half), axis=0))
            context_bias = cb_ref[h] * LOG2E
            top = jnp.maximum(jnp.concatenate(tops, axis=1), raw * factor + context_bias)
            return jnp.max(top, axis=0, keepdims=True), context_bias

        def finish_head(h, top, context_bias):
            slot = h % 2
            totals = []
            for side in range(2):
                cols = slice(side * half, (side + 1) * half)
                shift = jnp.broadcast_to(top[:, cols], (GRID_W, half))
                total = jnp.zeros((8, half), jnp.float32)
                for line in range(3 * REACH):
                    span_rows = slice(line * GRID_W, (line + 1) * GRID_W)
                    spot = tile_slot(line, side, first, last)
                    if isinstance(spot, int) and spot == blank:
                        prob[slot, span_rows, cols] = jnp.zeros((GRID_W, half), jnp.bfloat16)
                        continue
                    cell = jnp.exp2(score[slot, span_rows, cols] - shift)
                    total = total + jnp.sum(cell.reshape(-1, 8, half), axis=0)
                    prob[slot, span_rows, cols] = cell.astype(jnp.bfloat16)
                shift = shift - context_bias
                for c in range(ctx_count // GRID_W):
                    span_rows = slice(keys + c * GRID_W, keys + (c + 1) * GRID_W)
                    cell = jnp.exp2(score[slot, span_rows, cols] * factor - shift)
                    total = total + jnp.sum(cell.reshape(-1, 8, half), axis=0)
                    prob[slot, span_rows, cols] = cell.astype(jnp.bfloat16)
                totals.append(jnp.sum(total, axis=0, keepdims=True))
            out = dot32(vt[lanes_of(h, 0), pl.ds(at, keys)], prob[slot, :keys, :])
            out = out + dot32(ctxvt[lanes_of(h, 0), :], prob[slot, keys:, :])
            out = out * (1.0 / jnp.concatenate(totals, axis=1))
            att[pl.ds(at, span), lanes_of(h, 0)] = out.T.astype(jnp.bfloat16)

        state = scores(0)
        for h in range(heads):
            following = scores(h + 1) if h + 1 < heads else None
            finish_head(h, *state)
            state = following

    def hand(p):
        dest = p // per_dest
        local = p % per_dest
        src = pl.ds(pl.multiple_of(p * piece, piece), piece)
        dst = pl.ds(pl.multiple_of(local * piece, piece), piece)
        return remote(
            att.at[src, :], full.at[me_t, dst, :], att_send.at[p],
            att_recv.at[me_t * per_dest + local], "tp", dest,
        )

    def mirror(value, end):
        return jnp.where(upper, value, end - value)

    def attend_step(j, carry):
        b = mirror(lax.rem(j + 1, blocks), blocks - 1)
        fresh = mirror(lax.rem(j + 3, blocks + 2), blocks + 1)

        @pl.when((b == 0) & (me_s > 0))
        def _():
            down().wait_recv()

        @pl.when((b == blocks - 1) & (me_s < sp - 1))
        def _():
            up().wait_recv()

        prepare(fresh)
        first = jnp.where((b == 0) & (me_s == 0), 1, 0)
        last = jnp.where((b == blocks - 1) & (me_s == sp - 1), 1, 0)
        outer = first + last

        @pl.when(outer == 0)
        def _():
            attend(b, 0, 0)

        @pl.when(outer > 0)
        def _():
            attend(b, first, last)

        for i in range(per_block):
            p = b * per_block + i

            @pl.when(p // per_dest != me_t)
            def _():
                hand(p).start()

        return carry

    def far(k, i):
        near = lax.rem(chip + k, chips) * 2 + core
        other = lax.rem(chip + k, chips) * 2 + (1 - core)
        c = order(i, core)
        arrived(near, c)
        onward(k, c).start()
        project(near, c)
        c = order(i, 1 - core)
        arrived(other, c)
        project(other, c)

    send_early = chips == 2 and chunk_rows % 2 == 0 and chunks * piece_rows == chunk_rows
    if send_early:
        send_up(upper)
        send_down(lower)
        prepare(mirror(1, blocks + 1))
        prepare(mirror(2, blocks + 1))

        def overlap_step(i, carry):
            far(1, i)

            @pl.when(i == 0)
            def _():
                for k in range(1, sp):
                    from_sp(k, ctxbuf, ctx_send, ctx_recv)
                prepare_context()

            send_down(upper & (i == chunks - 2))
            send_up(lower & (i == chunks - 2))
            end = i + 1 + (i // (chunks - 1)) * (blocks - chunks)
            lax.fori_loop(i, end, attend_step, 0)
            return carry

        lax.fori_loop(0, chunks, overlap_step, 0)
    else:
        def far_step(i, carry):
            far(1 + i // chunks, lax.rem(i, chunks))
            return carry

        lax.fori_loop(0, (chips - 1) * chunks, far_step, 0)
        send_up(me_s >= 0)
        send_down(me_s >= 0)
        for k in range(1, sp):
            from_sp(k, ctxbuf, ctx_send, ctx_recv)
        prepare_context()
        prepare(mirror(1, blocks + 1))
        prepare(mirror(2, blocks + 1))
        lax.fori_loop(0, blocks, attend_step, 0)

    own = pl.ds(pl.multiple_of(me_t * count, count), count)
    full[me_t] = att[own, :]
    loads[3].wait()

    tile = HEAD_DIM * divisor(d // HEAD_DIM, 4)

    def finish(step, carry):
        j = mirror(per_dest - 1 - step, per_dest - 1)
        at = pl.ds(pl.multiple_of(j * piece, piece), piece)
        for k in range(1, tp):
            peer = lax.rem(me_t + k, tp)
            remote(
                full.at[peer, at, :], full.at[peer, at, :], att_send.at[0],
                att_recv.at[peer * per_dest + j], "tp", peer,
            ).wait_recv()

        def column(n, inner):
            lanes = pl.ds(pl.multiple_of(n * tile, tile), tile)
            result = dot32(full[0, at, :], wo[0:width, lanes])
            for t in range(1, tp):
                result = result + dot32(full[t, at, :], wo[t * width : (t + 1) * width, lanes])
            floats = tok[me_t, at, lanes].astype(jnp.float32)
            out_ref[at, lanes] = (floats + mods[2:3, lanes] * result).astype(jnp.bfloat16)
            return inner

        lax.fori_loop(0, d // tile, column, 0)
        return carry

    lax.fori_loop(0, per_dest, finish, 0)

    for c in range(chunks):
        beside(c).wait_send()
        for k in range(1, chips):
            across(k, c).wait_send()
            onward(k, c).wait_send()
    for k in range(1, sp):
        to_sp(k, modsp, msp_send, msp_recv).wait_send()
        to_sp(k, ctxbuf, ctx_send, ctx_recv).wait_send()
    for k in range(1, tp):
        to_tp(k).wait_send()

    def sent(p, carry):
        @pl.when(p // per_dest != me_t)
        def _():
            hand(p).wait_send()

        return carry

    lax.fori_loop(0, rows // piece_rows, sent, 0)

    @pl.when(me_s > 0)
    def _():
        up().wait_send()

    @pl.when(me_s < sp - 1)
    def _():
        down().wait_send()


def shards(
    resid,
    cond,
    mod_shift,
    mod_scale,
    mod_gate,
    norm_gain,
    context,
    w_query,
    w_key,
    w_value,
    query_gain,
    key_gain,
    offset_bias,
    context_bias,
    w_out,
):
    sp, tp = lax.axis_size("sp"), lax.axis_size("tp")
    count, d = resid.shape
    width = w_query.shape[1]
    heads = width // HEAD_DIM
    tokens = count * tp
    lanes = min(cond.shape[0], HEAD_DIM)
    chunk_rows = count // GRID_W
    chunks = divisor(chunk_rows, 3)
    pieces = chunk_rows // divisor(chunk_rows, 2)
    ctx_count = context.shape[0] * sp
    span = REACH * GRID_W
    chips = tp // 2
    bf, f32 = jnp.bfloat16, jnp.float32
    piece = mod_shift.shape[1]
    vmem = pl.BlockSpec(memory_space=pltpu.VMEM)
    hbm = pl.BlockSpec(memory_space=pl.ANY)
    sems = pltpu.SemaphoreType.DMA
    hops = max(1, (chips - 1) * chunks)
    return pl.pallas_call(
        functools.partial(layer_kernel, sp, tp, chunks),
        in_specs=[pl.BlockSpec(memory_space=pltpu.SMEM), hbm]
        + [vmem] * 6
        + [hbm] * 3
        + [vmem] * 3
        + [hbm],
        out_specs=vmem,
        out_shape=jax.ShapeDtypeStruct((count, d), bf),
        scratch_shapes=[
            pltpu.VMEM((tp, count, d), bf),
            pltpu.VMEM((d, width), bf),
            pltpu.VMEM((d, width), bf),
            pltpu.VMEM((d, width), bf),
            pltpu.VMEM((width * tp, d), bf),
            pltpu.VMEM((tokens, width), bf),
            pltpu.VMEM((tokens + 2 * REACH * GRID_W, 2 * width), bf),
            pltpu.VMEM((sp, context.shape[0], 2 * width), bf),
            pltpu.VMEM((offset_bias.shape[1], heads, 2 * GRID_W), f32),
            pltpu.VMEM((heads, 2 * WIN_ROWS + 3, GRID_W, 2 * GRID_W), f32),
            pltpu.VMEM((sp, 8, piece), f32),
            pltpu.VMEM((tp, 8, piece), f32),
            pltpu.VMEM((8, d), f32),
            pltpu.VMEM((tokens, width), bf),
            pltpu.VMEM((tp, count, width), bf),
            pltpu.VMEM((width, tokens + 2 * span), bf),
            pltpu.VMEM((width, ctx_count), bf),
            pltpu.VMEM((2, 3 * span + ctx_count, span), f32),
            pltpu.VMEM((2, 3 * span + ctx_count, span), bf),
            sems((5,)),
            sems((hops,)),
            sems((chunks,)),
            sems((hops,)),
            sems((tp * chunks,)),
            sems((sp,)),
            sems((sp,)),
            sems((tp,)),
            sems((tp,)),
            sems((sp,)),
            sems((sp,)),
            sems((2,)),
            sems((2,)),
            sems((tp * pieces,)),
            sems((tp * pieces,)),
        ],
        compiler_params=pltpu.CompilerParams(
            collective_id=0, has_side_effects=True, vmem_limit_bytes=VMEM_BYTES
        ),
        name="layer",
    )(
        context_bias, resid, cond.reshape(-1, lanes), mod_shift, mod_scale, mod_gate, norm_gain[None, :],
        context, w_query, w_key, w_value, query_gain[None, :], key_gain[None, :],
        jnp.transpose(offset_bias, (1, 0, 2)), w_out,
    )


def solution(mesh):
    in_specs = (
        P(("sp", "tp"), None),
        P("sp"),
        P("sp", "tp"),
        P("sp", "tp"),
        P("sp", "tp"),
        P(),
        P("sp", None),
        P(None, "tp"),
        P(None, "tp"),
        P(None, "tp"),
        P(),
        P(),
        P("tp", None, None),
        P("tp"),
        P(),
    )
    out_specs = P(("sp", "tp"), None)
    return jax.shard_map(shards, mesh=mesh, in_specs=in_specs, out_specs=out_specs, check_vma=False)
```

```python
import functools

import jax
import jax.numpy as jnp
from jax import lax
from jax.experimental import pallas as pl
from jax.experimental.pallas import tpu as pltpu
from jax.sharding import PartitionSpec as P

HEAD_DIM = 128
GRID_W = 64
WIN_ROWS = 8
WIN_COLS = 16
REACH = WIN_ROWS // 2
EPS = 1e-06
LOG2E = 1.4426950408889634
MASKED = -1e30
VMEM_BYTES = 56 * 1024 * 1024


def dot32(a, b):
    return jnp.dot(a, b, preferred_element_type=jnp.float32)


def dot_t(a, b):
    return lax.dot_general(a, b, (((1,), (1,)), ((), ())), preferred_element_type=jnp.float32)


def divisor(count, most):
    return max(d for d in range(1, most + 1) if count % d == 0)


def normed_tokens(rows, gain):
    floats = rows.astype(jnp.float32)
    inverse = lax.rsqrt(jnp.mean(floats * floats, axis=-1, keepdims=True) + EPS)
    return floats * inverse * gain


def store_heads(out_ref, at, values, gain):
    count = values.shape[0]
    for h in range(values.shape[1] // HEAD_DIM):
        part = values[:, h * HEAD_DIM : (h + 1) * HEAD_DIM]
        part = part * lax.rsqrt(jnp.mean(part * part, axis=-1, keepdims=True) + EPS) * gain
        out_ref[pl.ds(at, count), h * HEAD_DIM : (h + 1) * HEAD_DIM] = part.astype(jnp.bfloat16)


def fill_bias(ob_ref, table, h):
    rows = 2 * WIN_ROWS - 1
    lanes = 2 * GRID_W
    lane = lax.broadcasted_iota(jnp.int32, (lanes, lanes), 1)
    line = lax.broadcasted_iota(jnp.int32, (lanes, lanes), 0)
    query = line % GRID_W
    begin = jnp.clip(query - WIN_COLS // 2, 0, GRID_W - WIN_COLS)
    valid = (lane >= begin) & (lane < begin + WIN_COLS)

    def spread(r):
        row = jnp.broadcast_to(ob_ref[r, pl.ds(h, 1), :], (GRID_W, lanes))
        return pltpu.roll(row, lanes - (WIN_COLS - 1), 1, stride=1, stride_axis=0)

    masked = jnp.full((GRID_W, lanes), MASKED, jnp.float32)

    def put(slot, first, second):
        both = jnp.concatenate([first, second], axis=0) * LOG2E
        both = jnp.where(valid, both, MASKED)
        table[h, slot] = both.T[:GRID_W]

    low, high = REACH - 1, REACH - 1 + WIN_ROWS
    spreads = [spread(r) for r in range(rows)]
    for r in range(rows + 1):
        put(r, spreads[r] if r < rows else masked, spreads[r - 1] if r > 0 else masked)
    put(rows + 1, spreads[low], masked)
    put(rows + 2, masked, spreads[high - 1])
    table[h, rows + 3] = masked


def layer_kernel(
    sp, tp, chunks, cb_hbm, resid, cond_hbm, mshift_hbm, mscale_hbm, mgate_hbm, gain_hbm, context_hbm,
    wq_hbm, wk_hbm, wv_hbm, qg_hbm, kg_hbm, ob_hbm, wo_hbm, out_ref,
    cb, cond, mshift, mscale, mgate, gain_ref, context, qg, kg, ob_in,
    tok, wq, wk, wv, wo, qbuf, kvbuf, ctxbuf, ob_ref, table, modsp, modtp, mods, att, full,
    vt, ctxvt, score, prob, partial,
    load_sem, tok_send, pair_send, fwd_send, tok_recv, msp_send, msp_recv, mtp_send, mtp_recv,
    ctx_send, ctx_recv, halo_send, halo_recv, att_send, att_recv,
):
    me_s, me_t = lax.axis_index("sp"), lax.axis_index("tp")
    count, d = resid.shape
    chunk = count // chunks
    width = wq.shape[1]
    heads = width // HEAD_DIM
    tokens = count * tp
    rows = tokens // GRID_W
    total_rows = rows * sp
    first = me_s * rows
    chips = tp // 2
    chip, core = me_t // 2, me_t % 2
    pair = chip * 2 + (1 - core)

    def remote(src, dst, send, recv, axis, peer):
        return pltpu.make_async_remote_copy(
            src_ref=src, dst_ref=dst, send_sem=send, recv_sem=recv,
            device_id={axis: peer}, device_id_type=pl.DeviceIdType.MESH,
        )

    barrier = pltpu.get_barrier_semaphore()
    for k in range(1, sp):
        pl.semaphore_signal(
            barrier, inc=1, device_id={"sp": lax.rem(me_s + k, sp)},
            device_id_type=pl.DeviceIdType.MESH,
        )
    for k in range(1, tp):
        pl.semaphore_signal(
            barrier, inc=1, device_id={"tp": lax.rem(me_t + k, tp)},
            device_id_type=pl.DeviceIdType.MESH,
        )

    def load(index, src, dst):
        return pltpu.make_async_copy(src, dst, load_sem.at[index])

    small = [
        load(i, src, dst)
        for i, (src, dst) in enumerate(
            (
                (cond_hbm, cond), (mshift_hbm, mshift), (mscale_hbm, mscale), (mgate_hbm, mgate),
                (context_hbm, context), (gain_hbm, gain_ref), (kg_hbm, kg), (qg_hbm, qg),
                (ob_hbm, ob_in), (cb_hbm, cb),
            )
        )
    ]
    base = len(small)
    load_k, load_v = load(base, wk_hbm, wk), load(base + 1, wv_hbm, wv)
    load_q, load_o = load(base + 2, wq_hbm, wq), load(base + 3, wo_hbm, wo)
    load_tokens = load(base + 4, resid, tok.at[me_t])
    for copy in small[:6] + [load_tokens, load_k, load_v] + small[6:] + [load_q]:
        copy.start()
    pl.semaphore_wait(barrier, sp + tp - 2)

    def part(block, c):
        return tok.at[block, pl.ds(pl.multiple_of(c * chunk, chunk), chunk), :]

    def mine(c):
        return resid.at[pl.ds(pl.multiple_of(c * chunk, chunk), chunk), :]

    chunk_rows = rows // tp
    weave = chips == 2 and chunks == 3 and chunk_rows == 6
    is_low = chip // ((chips + 1) // 2)

    def plan(i, side, low):
        if not weave:
            return 0, i
        role = low * side + (1 - low) * (1 - side)
        swap = jnp.where(i == 1 + role, 1, 0)
        c = jnp.where(i == 0, chunks - 1, role)
        return swap, low * c + (1 - low) * (chunks - 1 - c)

    def across(k, i):
        peer = lax.rem(chip + k, chips) * 2 + core
        swap, c = plan(i, core, is_low)
        owner = chip * 2 + (core + swap) % 2
        return remote(
            part(owner, c), part(owner, c), tok_send.at[(k - 1) * chunks + i],
            tok_recv.at[owner * chunks + c], "tp", peer,
        )

    def across_part(k, begin, size, src):
        peer = lax.rem(chip + k, chips) * 2 + core
        c = plan(0, core, is_low)[1]
        at = pl.ds(pl.multiple_of(c * chunk + begin, 16), size)
        return remote(
            src.at[at, :], tok.at[me_t, at, :], tok_send.at[(k - 1) * chunks],
            tok_recv.at[me_t * chunks + c], "tp", peer,
        )

    def beside(c):
        return remote(
            mine(c), part(me_t, c), pair_send.at[c], tok_recv.at[me_t * chunks + c], "tp", pair
        )

    def onward(k, i, block, c):
        return remote(
            part(block, c), part(block, c), fwd_send.at[(k - 1) * chunks + i],
            tok_recv.at[block * chunks + c], "tp", pair,
        )

    def arrived(block, c):
        remote(
            part(block, c), part(block, c), pair_send.at[0], tok_recv.at[block * chunks + c],
            "tp", pair,
        ).wait_recv()

    early = chunk * 3 // 128 * 16 if chunk >= 128 else chunk // 2
    for k in range(1, chips):
        across_part(k, 0, early, resid).start()
    for c in range(chunks):
        beside(c).start()

    for copy in small[:4]:
        copy.wait()
    lifted = cond[...].astype(jnp.float32)
    lifted = (lifted / (1.0 + jnp.exp(-lifted))).astype(jnp.bfloat16)
    lanes = lifted.shape[1]
    for i, m in enumerate((mshift, mscale, mgate)):
        sums = []
        for r in range(lifted.shape[0]):
            line = jnp.broadcast_to(lifted[r : r + 1, :], (16, lanes))
            sums.append(dot32(line, m[r * lanes : (r + 1) * lanes, :])[0:1])
        modsp[me_s, i : i + 1, :] = functools.reduce(jnp.add, sums)
    modsp[me_s, 3:8, :] = jnp.zeros((5, modsp.shape[2]), jnp.float32)

    def to_sp(k, buf, send, recv):
        return remote(
            buf.at[me_s], buf.at[me_s], send.at[k - 1], recv.at[me_s], "sp", lax.rem(me_s + k, sp)
        )

    def from_sp(k, buf, send, recv):
        peer = lax.rem(me_s + k, sp)
        remote(buf.at[peer], buf.at[peer], send.at[k - 1], recv.at[peer], "sp", peer).wait_recv()

    for k in range(1, sp):
        to_sp(k, modsp, msp_send, msp_recv).start()

    for copy in small[4:7]:
        copy.wait()
    load_k.wait()
    load_v.wait()
    normed = normed_tokens(context[...], gain_ref[...]).astype(jnp.bfloat16)
    own = ctxbuf.at[me_s]
    store_heads(own, 0, dot32(normed, wk[...]), kg[...])
    own[:, width:] = dot32(normed, wv[...]).astype(jnp.bfloat16)
    for k in range(1, sp):
        to_sp(k, ctxbuf, ctx_send, ctx_recv).start()

    for copy in small[7:]:
        copy.wait()
    ob_ref[...] = jnp.zeros_like(ob_ref)
    ob_ref[:, :, : ob_in.shape[2]] = ob_in[...]

    def fill(h, carry):
        fill_bias(ob_ref, table, h)
        return carry

    lax.fori_loop(0, heads // 2, fill, 0)

    for k in range(1, sp):
        from_sp(k, modsp, msp_send, msp_recv)
    summed = modsp[0]
    for s in range(1, sp):
        summed = summed + modsp[s]
    modtp[me_t] = summed

    def to_tp(k):
        return remote(
            modtp.at[me_t], modtp.at[me_t], mtp_send.at[k - 1], mtp_recv.at[me_t], "tp",
            lax.rem(me_t + k, tp),
        )

    for k in range(1, tp):
        to_tp(k).start()
    load_tokens.wait()
    for k in range(1, chips):
        across_part(k, early, chunk - early, tok.at[me_t]).start()
    for c in range(chunks):
        arrived(pair, c)
    for i in range(1, chunks):
        for k in range(1, chips):
            across(k, i).start()

    lax.fori_loop(heads // 2, heads, fill, 0)

    load_o.start()
    load_q.wait()
    for k in range(1, tp):
        peer = lax.rem(me_t + k, tp)
        remote(
            modtp.at[peer], modtp.at[peer], mtp_send.at[k - 1], mtp_recv.at[peer], "tp", peer
        ).wait_recv()
    piece = modtp.shape[2]
    for t in range(tp):
        mods[:, t * piece : (t + 1) * piece] = modtp[t]

    edge = REACH * GRID_W

    def project(block, c):
        values = tok[block, pl.ds(pl.multiple_of(c * chunk, chunk), chunk), :]
        normed = normed_tokens(values, gain_ref[...]) * (1.0 + mods[1:2, :]) + mods[0:1, :]
        normed = normed.astype(jnp.bfloat16)
        at = pl.multiple_of(block * count + c * chunk, chunk)
        store_heads(qbuf, at, dot32(normed, wq[...]), qg[...])
        at = pl.multiple_of(edge + block * count + c * chunk, GRID_W)
        store_heads(kvbuf, at, dot32(normed, wk[...]), kg[...])
        kvbuf[pl.ds(at, chunk), width:] = dot32(normed, wv[...]).astype(jnp.bfloat16)

    def local_step(c, carry):
        project(me_t, c)
        return carry

    lax.fori_loop(0, chunks, local_step, 0)

    def pair_step(c, carry):
        project(pair, c)
        return carry

    lax.fori_loop(0, chunks, pair_step, 0)

    def up():
        return remote(
            kvbuf.at[pl.ds(edge, edge), :], kvbuf.at[pl.ds(edge + tokens, edge), :],
            halo_send.at[0], halo_recv.at[0], "sp", me_s - 1,
        )

    def down():
        return remote(
            kvbuf.at[pl.ds(tokens, edge), :], kvbuf.at[pl.ds(0, edge), :],
            halo_send.at[1], halo_recv.at[1], "sp", me_s + 1,
        )

    upper = chip < (chips + 1) // 2
    lower = jnp.logical_not(upper)

    def send_up(when):
        @pl.when(when & (me_s > 0))
        def _():
            up().start()

    def send_down(when):
        @pl.when(when & (me_s < sp - 1))
        def _():
            down().start()

    @pl.when(me_s == 0)
    def _():
        kvbuf[0:edge, :] = jnp.zeros((edge, 2 * width), jnp.bfloat16)

    @pl.when(me_s == sp - 1)
    def _():
        kvbuf[edge + tokens :, :] = jnp.zeros((edge, 2 * width), jnp.bfloat16)

    ctx_count = ctxbuf.shape[0] * ctxbuf.shape[1]
    factor = HEAD_DIM ** (-0.5) * LOG2E
    span = edge
    blocks = rows // REACH
    half = 2 * GRID_W
    keys = 3 * span
    piece_rows = divisor(chunk_rows, 2) if REACH % 2 == 0 else 1
    piece = piece_rows * GRID_W
    per_dest = chunk_rows // piece_rows
    per_block = REACH // piece_rows
    bias_rows = 2 * WIN_ROWS - 1
    plain = list(range(bias_rows + 1))
    lead, trail, blank = bias_rows + 1, bias_rows + 2, bias_rows + 3

    def prepare(kb):
        at = pl.ds(pl.multiple_of(kb * span, span), span)
        vt[:, at] = kvbuf[at, width:].T

    def prepare_context():
        values = ctxbuf[:, :, width:].reshape(ctx_count, width)
        ctxvt[...] = values.T

    def tile_slot(line, side, first, last):
        r = line + REACH - 1 - 2 * side
        low, high = REACH - 1, REACH - 1 + WIN_ROWS
        inner = lead if r == low else trail if r == high else r if low < r < high else blank
        at_first = r if line >= REACH else blank
        at_last = r if line < 2 * REACH else blank
        if inner == at_first == at_last:
            return inner
        return inner + first * (at_first - inner) + last * (at_last - inner)

    def attend(b, first, last):
        at = pl.multiple_of(b * span, span)
        heads = width // HEAD_DIM

        def lanes_of(h, base):
            return slice(base + h * HEAD_DIM, base + (h + 1) * HEAD_DIM)

        def scores(h):
            queries = qbuf[pl.ds(at, span), lanes_of(h, 0)]
            slot = h % 2
            tops = [jnp.full((8, half), MASKED, jnp.float32) for _ in range(2)]
            for kb in range(3):
                part = dot_t(kvbuf[pl.ds(at + kb * span, span), lanes_of(h, 0)], queries)
                for i in range(REACH):
                    line = kb * REACH + i
                    for side in range(2):
                        spot = tile_slot(line, side, first, last)
                        if isinstance(spot, int) and spot == blank:
                            continue
                        cell = part[i * GRID_W : (i + 1) * GRID_W, side * half : (side + 1) * half]
                        cell = cell * factor + table[h, spot]
                        score[slot, line * GRID_W : (line + 1) * GRID_W, side * half : (side + 1) * half] = cell
                        tops[side] = jnp.maximum(tops[side], jnp.max(cell.reshape(-1, 8, half), axis=0))
            raw = jnp.full((8, 2 * half), -jnp.inf, jnp.float32)
            for c in range(ctx_count // span):
                ctx_key = ctxbuf[c * span // ctxbuf.shape[1] : (c + 1) * span // ctxbuf.shape[1], :, lanes_of(h, 0)]
                part = dot_t(ctx_key.reshape(span, HEAD_DIM), queries)
                score[slot, keys + c * span : keys + (c + 1) * span, :] = part
                raw = jnp.maximum(raw, jnp.max(part.reshape(-1, 8, 2 * half), axis=0))
            context_bias = cb[0:1, h : h + 1] * LOG2E
            top = jnp.maximum(jnp.concatenate(tops, axis=1), raw * factor + context_bias)
            return jnp.max(top, axis=0, keepdims=True), context_bias

        def finish_head(h, top, context_bias):
            slot = h % 2
            totals = []
            for side in range(2):
                cols = slice(side * half, (side + 1) * half)
                shift = jnp.broadcast_to(top[:, cols], (GRID_W, half))
                total = jnp.zeros((8, half), jnp.float32)
                for line in range(3 * REACH):
                    span_rows = slice(line * GRID_W, (line + 1) * GRID_W)
                    spot = tile_slot(line, side, first, last)
                    if isinstance(spot, int) and spot == blank:
                        prob[slot, span_rows, cols] = jnp.zeros((GRID_W, half), jnp.bfloat16)
                        continue
                    cell = jnp.exp2(score[slot, span_rows, cols] - shift)
                    total = total + jnp.sum(cell.reshape(-1, 8, half), axis=0)
                    prob[slot, span_rows, cols] = cell.astype(jnp.bfloat16)
                shift = shift - context_bias
                for c in range(ctx_count // GRID_W):
                    span_rows = slice(keys + c * GRID_W, keys + (c + 1) * GRID_W)
                    cell = jnp.exp2(score[slot, span_rows, cols] * factor - shift)
                    total = total + jnp.sum(cell.reshape(-1, 8, half), axis=0)
                    prob[slot, span_rows, cols] = cell.astype(jnp.bfloat16)
                totals.append(jnp.sum(total, axis=0, keepdims=True))
            out = dot32(vt[lanes_of(h, 0), pl.ds(at, keys)], prob[slot, :keys, :])
            out = out + dot32(ctxvt[lanes_of(h, 0), :], prob[slot, keys:, :])
            out = out * (1.0 / jnp.concatenate(totals, axis=1))
            att[pl.ds(at, span), lanes_of(h, 0)] = out.T.astype(jnp.bfloat16)

        state = scores(0)
        for h in range(heads):
            following = scores(h + 1) if h + 1 < heads else None
            finish_head(h, *state)
            state = following

    def hand(p):
        dest = p // per_dest
        local = p % per_dest
        src = pl.ds(pl.multiple_of(p * piece, piece), piece)
        dst = pl.ds(pl.multiple_of(local * piece, piece), piece)
        return remote(
            att.at[src, :], full.at[me_t, dst, :], att_send.at[p],
            att_recv.at[me_t * per_dest + local], "tp", dest,
        )

    def mirror(value, end):
        return jnp.where(upper, value, end - value)

    def wait_top():
        @pl.when(me_s > 0)
        def _():
            down().wait_recv()

    def wait_bottom():
        @pl.when(me_s < sp - 1)
        def _():
            up().wait_recv()

    def attend_block(b):
        first = jnp.where((b == 0) & (me_s == 0), 1, 0)
        last = jnp.where((b == blocks - 1) & (me_s == sp - 1), 1, 0)
        outer = first + last

        @pl.when(outer == 0)
        def _():
            attend(b, 0, 0)

        @pl.when(outer > 0)
        def _():
            attend(b, first, last)

        for i in range(per_block):
            p = b * per_block + jnp.where(upper, per_block - 1 - i, i)

            @pl.when(p // per_dest != me_t)
            def _():
                hand(p).start()

    def far(k, i):
        far_chip = lax.rem(chip + k, chips)
        low = far_chip // ((chips + 1) // 2)
        swap, c = plan(i, core, low)
        block = far_chip * 2 + (core + swap) % 2
        arrived(block, c)
        onward(k, i, block, c).start()
        project(block, c)
        swap, c = plan(i, 1 - core, low)
        block = far_chip * 2 + (1 - core + swap) % 2
        arrived(block, c)
        project(block, c)

    def context_ready():
        for k in range(1, sp):
            from_sp(k, ctxbuf, ctx_send, ctx_recv)
        prepare_context()

    if weave:
        send_up(upper)
        send_down(lower)
        prepare(mirror(1, blocks + 1))
        prepare(mirror(2, blocks + 1))

        def attend_step(j, carry):
            b = jnp.where(j == 0, 1, jnp.where(j == blocks - 1, 0, blocks - j))
            fresh = jnp.where(j == 0, 3, jnp.where(j == 1, blocks + 1, jnp.where(j == 2, 4, 0)))
            b = mirror(b, blocks - 1)

            @pl.when(b == 0)
            def _():
                wait_top()

            @pl.when(b == blocks - 1)
            def _():
                wait_bottom()

            @pl.when((j < 3) | (j == blocks - 1))
            def _():
                prepare(mirror(fresh, blocks + 1))

            attend_block(b)
            return carry

        def weave_step(i, carry):
            far(1, i)

            @pl.when(i == 0)
            def _():
                context_ready()

            send_down(upper & (i == chunks - 2))
            send_up(lower & (i == chunks - 2))

            @pl.when(i == chunks - 2)
            def _():
                prepare(mirror(blocks - 1, blocks + 1))
                prepare(mirror(blocks, blocks + 1))

            end = i + 1 + (i // (chunks - 1)) * (blocks - chunks)
            lax.fori_loop(i, end, attend_step, 0)
            return carry

        lax.fori_loop(0, chunks, weave_step, 0)
    else:
        def far_step(i, carry):
            far(1 + i // chunks, lax.rem(i, chunks))
            return carry

        def prepare_step(kb, carry):
            prepare(kb)
            return carry

        def plain_step(b, carry):
            attend_block(b)
            return carry

        lax.fori_loop(0, (chips - 1) * chunks, far_step, 0)
        send_up(me_s >= 0)
        send_down(me_s >= 0)
        context_ready()
        wait_top()
        wait_bottom()
        lax.fori_loop(0, blocks + 2, prepare_step, 0)
        lax.fori_loop(0, blocks, plain_step, 0)

    own = pl.ds(pl.multiple_of(me_t * count, count), count)
    full[me_t] = att[own, :]
    load_o.wait()

    tile = HEAD_DIM * divisor(d // HEAD_DIM, 4)

    def await_piece(peer, j):
        at = pl.ds(pl.multiple_of(j * piece, piece), piece)
        remote(
            full.at[peer, at, :], full.at[peer, at, :], att_send.at[0],
            att_recv.at[peer * per_dest + j], "tp", peer,
        ).wait_recv()

    def project_out(peer, at, lanes):
        return dot32(full[peer, at, :], wo[pl.ds(pl.multiple_of(peer * width, width), width), lanes])

    def near_piece(step, carry):
        j = mirror(per_dest - 1 - step, per_dest - 1)
        at = pl.ds(pl.multiple_of(j * piece, piece), piece)
        await_piece(pair, j)

        def column(n, inner):
            lanes = pl.ds(pl.multiple_of(n * tile, tile), tile)
            partial[at, lanes] = project_out(me_t, at, lanes) + project_out(pair, at, lanes)
            return inner

        lax.fori_loop(0, d // tile, column, 0)
        return carry

    def far_piece(step, carry):
        j = mirror(step, per_dest - 1)
        at = pl.ds(pl.multiple_of(j * piece, piece), piece)
        peers = [
            lax.rem(chip + k, chips) * 2 + side for k in range(1, chips) for side in range(2)
        ]
        for peer in peers:
            await_piece(peer, j)

        def column(n, inner):
            lanes = pl.ds(pl.multiple_of(n * tile, tile), tile)
            result = partial[at, lanes]
            for peer in peers:
                result = result + project_out(peer, at, lanes)
            floats = tok[me_t, at, lanes].astype(jnp.float32)
            out_ref[at, lanes] = (floats + mods[2:3, lanes] * result).astype(jnp.bfloat16)
            return inner

        lax.fori_loop(0, d // tile, column, 0)
        return carry

    lax.fori_loop(0, per_dest, near_piece, 0)
    lax.fori_loop(0, per_dest, far_piece, 0)

    for c in range(chunks):
        beside(c).wait_send()
        for k in range(1, chips):
            across(k, c).wait_send()
            onward(k, c, me_t, c).wait_send()
    for k in range(1, sp):
        to_sp(k, modsp, msp_send, msp_recv).wait_send()
        to_sp(k, ctxbuf, ctx_send, ctx_recv).wait_send()
    for k in range(1, tp):
        to_tp(k).wait_send()

    def sent(p, carry):
        @pl.when(p // per_dest != me_t)
        def _():
            hand(p).wait_send()

        return carry

    lax.fori_loop(0, rows // piece_rows, sent, 0)

    @pl.when(me_s > 0)
    def _():
        up().wait_send()

    @pl.when(me_s < sp - 1)
    def _():
        down().wait_send()


def shards(
    resid,
    cond,
    mod_shift,
    mod_scale,
    mod_gate,
    norm_gain,
    context,
    w_query,
    w_key,
    w_value,
    query_gain,
    key_gain,
    offset_bias,
    context_bias,
    w_out,
):
    sp, tp = lax.axis_size("sp"), lax.axis_size("tp")
    count, d = resid.shape
    width = w_query.shape[1]
    heads = width // HEAD_DIM
    tokens = count * tp
    lanes = min(cond.shape[0], HEAD_DIM)
    chunk_rows = count // GRID_W
    chunks = divisor(chunk_rows, 3)
    pieces = chunk_rows // divisor(chunk_rows, 2)
    ctx_count = context.shape[0] * sp
    span = REACH * GRID_W
    chips = tp // 2
    bf, f32 = jnp.bfloat16, jnp.float32
    piece = mod_shift.shape[1]
    vmem = pl.BlockSpec(memory_space=pltpu.VMEM)
    hbm = pl.BlockSpec(memory_space=pltpu.HBM)
    sems = pltpu.SemaphoreType.DMA
    hops = max(1, (chips - 1) * chunks)
    return pl.pallas_call(
        functools.partial(layer_kernel, sp, tp, chunks),
        in_specs=[hbm] * 15,
        out_specs=vmem,
        out_shape=pltpu.VMEM((count, d), bf),
        scratch_shapes=[
            pltpu.VMEM((1, heads), f32),
            pltpu.VMEM((cond.shape[0] // lanes, lanes), bf),
            pltpu.VMEM(mod_shift.shape, bf),
            pltpu.VMEM(mod_scale.shape, bf),
            pltpu.VMEM(mod_gate.shape, bf),
            pltpu.VMEM((1, d), f32),
            pltpu.VMEM(context.shape, bf),
            pltpu.VMEM((1, HEAD_DIM), f32),
            pltpu.VMEM((1, HEAD_DIM), f32),
            pltpu.VMEM((offset_bias.shape[1], heads, offset_bias.shape[2]), f32),
            pltpu.VMEM((tp, count, d), bf),
            pltpu.VMEM((d, width), bf),
            pltpu.VMEM((d, width), bf),
            pltpu.VMEM((d, width), bf),
            pltpu.VMEM((width * tp, d), bf),
            pltpu.VMEM((tokens, width), bf),
            pltpu.VMEM((tokens + 2 * REACH * GRID_W, 2 * width), bf),
            pltpu.VMEM((sp, context.shape[0], 2 * width), bf),
            pltpu.VMEM((offset_bias.shape[1], heads, 2 * GRID_W), f32),
            pltpu.VMEM((heads, 2 * WIN_ROWS + 3, GRID_W, 2 * GRID_W), f32),
            pltpu.VMEM((sp, 8, piece), f32),
            pltpu.VMEM((tp, 8, piece), f32),
            pltpu.VMEM((8, d), f32),
            pltpu.VMEM((tokens, width), bf),
            pltpu.VMEM((tp, count, width), bf),
            pltpu.VMEM((width, tokens + 2 * span), bf),
            pltpu.VMEM((width, ctx_count), bf),
            pltpu.VMEM((2, 3 * span + ctx_count, span), f32),
            pltpu.VMEM((2, 3 * span + ctx_count, span), bf),
            pltpu.VMEM((count, d), f32),
            sems((15,)),
            sems((hops,)),
            sems((chunks,)),
            sems((hops,)),
            sems((tp * chunks,)),
            sems((sp,)),
            sems((sp,)),
            sems((tp,)),
            sems((tp,)),
            sems((sp,)),
            sems((sp,)),
            sems((2,)),
            sems((2,)),
            sems((tp * pieces,)),
            sems((tp * pieces,)),
        ],
        compiler_params=pltpu.CompilerParams(
            collective_id=0, has_side_effects=True, vmem_limit_bytes=VMEM_BYTES
        ),
        name="layer",
    )(
        context_bias[None, :], resid, cond.reshape(-1, lanes), mod_shift, mod_scale, mod_gate, norm_gain[None, :],
        context, w_query, w_key, w_value, query_gain[None, :], key_gain[None, :],
        jnp.transpose(offset_bias, (1, 0, 2)), w_out,
    )


def solution(mesh):
    in_specs = (
        P(("sp", "tp"), None),
        P("sp"),
        P("sp", "tp"),
        P("sp", "tp"),
        P("sp", "tp"),
        P(),
        P("sp", None),
        P(None, "tp"),
        P(None, "tp"),
        P(None, "tp"),
        P(),
        P(),
        P("tp", None, None),
        P("tp"),
        P(),
    )
    out_specs = P(("sp", "tp"), None)
    return jax.shard_map(shards, mesh=mesh, in_specs=in_specs, out_specs=out_specs, check_vma=False)
```

```python
import functools

import jax
import jax.numpy as jnp
from jax import lax
from jax.experimental import pallas as pl
from jax.experimental.pallas import tpu as pltpu
from jax.sharding import PartitionSpec as P

HEAD_DIM = 128
GRID_W = 64
WIN_ROWS = 8
WIN_COLS = 16
REACH = WIN_ROWS // 2
EPS = 1e-06
LOG2E = 1.4426950408889634
MASKED = -1e30
VMEM_BYTES = 56 * 1024 * 1024


def dot32(a, b):
    return jnp.dot(a, b, preferred_element_type=jnp.float32)


def dot_t(a, b):
    return lax.dot_general(a, b, (((1,), (1,)), ((), ())), preferred_element_type=jnp.float32)


def divisor(count, most):
    return max(d for d in range(1, most + 1) if count % d == 0)


def normed_tokens(rows, gain):
    floats = rows.astype(jnp.float32)
    inverse = lax.rsqrt(jnp.mean(floats * floats, axis=-1, keepdims=True) + EPS)
    return floats * inverse * gain


def store_heads(out_ref, at, values, gain):
    count = values.shape[0]
    for h in range(values.shape[1] // HEAD_DIM):
        part = values[:, h * HEAD_DIM : (h + 1) * HEAD_DIM]
        part = part * lax.rsqrt(jnp.mean(part * part, axis=-1, keepdims=True) + EPS) * gain
        out_ref[pl.ds(at, count), h * HEAD_DIM : (h + 1) * HEAD_DIM] = part.astype(jnp.bfloat16)


def fill_bias(ob_ref, table, h):
    rows = 2 * WIN_ROWS - 1
    lanes = 2 * GRID_W
    lane = lax.broadcasted_iota(jnp.int32, (lanes, lanes), 1)
    line = lax.broadcasted_iota(jnp.int32, (lanes, lanes), 0)
    query = line % GRID_W
    begin = jnp.clip(query - WIN_COLS // 2, 0, GRID_W - WIN_COLS)
    valid = (lane >= begin) & (lane < begin + WIN_COLS)

    def spread(r):
        row = jnp.broadcast_to(ob_ref[r, pl.ds(h, 1), :], (GRID_W, lanes))
        return pltpu.roll(row, lanes - (WIN_COLS - 1), 1, stride=1, stride_axis=0)

    masked = jnp.full((GRID_W, lanes), MASKED, jnp.float32)

    def put(slot, first, second):
        both = jnp.concatenate([first, second], axis=0) * LOG2E
        both = jnp.where(valid, both, MASKED)
        table[h, slot] = both.T[:GRID_W]

    low, high = REACH - 1, REACH - 1 + WIN_ROWS
    spreads = [spread(r) for r in range(rows)]
    for r in range(rows + 1):
        put(r, spreads[r] if r < rows else masked, spreads[r - 1] if r > 0 else masked)
    put(rows + 1, spreads[low], masked)
    put(rows + 2, masked, spreads[high - 1])
    table[h, rows + 3] = masked


def layer_kernel(
    sp, tp, chunks, cb_hbm, resid, cond_hbm, mshift_hbm, mscale_hbm, mgate_hbm, gain_hbm, context_hbm,
    wq_hbm, wk_hbm, wv_hbm, qg_hbm, kg_hbm, ob_hbm, wo_hbm, out_ref,
    cb, cond, mshift, mscale, mgate, gain_ref, context, qg, kg, ob_in,
    tok, wq, wk, wv, wo, qbuf, kvbuf, ctxbuf, ob_ref, table, modsp, modtp, mods, att, full,
    vt, ctxvt, score, prob, partial,
    load_sem, tok_send, pair_send, fwd_send, tok_recv, msp_send, msp_recv, mtp_send, mtp_recv,
    ctx_send, ctx_recv, halo_send, halo_recv, att_send, att_recv,
):
    me_s, me_t = lax.axis_index("sp"), lax.axis_index("tp")
    count, d = resid.shape
    chunk = count // chunks
    width = wq.shape[1]
    heads = width // HEAD_DIM
    tokens = count * tp
    rows = tokens // GRID_W
    total_rows = rows * sp
    first = me_s * rows
    chips = tp // 2
    chip, core = me_t // 2, me_t % 2
    pair = chip * 2 + (1 - core)

    def remote(src, dst, send, recv, axis, peer):
        return pltpu.make_async_remote_copy(
            src_ref=src, dst_ref=dst, send_sem=send, recv_sem=recv,
            device_id={axis: peer}, device_id_type=pl.DeviceIdType.MESH,
        )

    barrier = pltpu.get_barrier_semaphore()
    for k in range(1, sp):
        pl.semaphore_signal(
            barrier, inc=1, device_id={"sp": lax.rem(me_s + k, sp)},
            device_id_type=pl.DeviceIdType.MESH,
        )
    for k in range(1, tp):
        pl.semaphore_signal(
            barrier, inc=1, device_id={"tp": lax.rem(me_t + k, tp)},
            device_id_type=pl.DeviceIdType.MESH,
        )

    def load(index, src, dst):
        return pltpu.make_async_copy(src, dst, load_sem.at[index])

    small = [
        load(i, src, dst)
        for i, (src, dst) in enumerate(
            (
                (cond_hbm, cond), (mshift_hbm, mshift), (mscale_hbm, mscale), (mgate_hbm, mgate),
                (context_hbm, context), (gain_hbm, gain_ref), (kg_hbm, kg), (qg_hbm, qg),
                (ob_hbm, ob_in), (cb_hbm, cb),
            )
        )
    ]
    base = len(small)
    load_k, load_v = load(base, wk_hbm, wk), load(base + 1, wv_hbm, wv)
    load_q, load_o = load(base + 2, wq_hbm, wq), load(base + 3, wo_hbm, wo)
    load_tokens = load(base + 4, resid, tok.at[me_t])
    for copy in small[:6] + [load_tokens, load_k, load_v] + small[6:] + [load_q]:
        copy.start()
    pl.semaphore_wait(barrier, sp + tp - 2)

    def part(block, c):
        return tok.at[block, pl.ds(pl.multiple_of(c * chunk, chunk), chunk), :]

    def mine(c):
        return resid.at[pl.ds(pl.multiple_of(c * chunk, chunk), chunk), :]

    chunk_rows = rows // tp
    weave = chips == 2 and chunks == 3 and chunk_rows == 6

    def plan(i, side):
        if not weave:
            return 0, i
        return jnp.where(i == 1 + side, 1, 0), jnp.where(i == 0, chunks - 1, side)

    def across(k, i):
        peer = lax.rem(chip + k, chips) * 2 + core
        swap, c = plan(i, core)
        owner = chip * 2 + (core + swap) % 2
        return remote(
            part(owner, c), part(owner, c), tok_send.at[(k - 1) * chunks + i],
            tok_recv.at[owner * chunks + c], "tp", peer,
        )

    def across_part(k, begin, size, src):
        peer = lax.rem(chip + k, chips) * 2 + core
        c = plan(0, core)[1]
        at = pl.ds(pl.multiple_of(c * chunk + begin, 16), size)
        return remote(
            src.at[at, :], tok.at[me_t, at, :], tok_send.at[(k - 1) * chunks],
            tok_recv.at[me_t * chunks + c], "tp", peer,
        )

    def beside(c):
        return remote(
            mine(c), part(me_t, c), pair_send.at[c], tok_recv.at[me_t * chunks + c], "tp", pair
        )

    def onward(k, i, block, c):
        return remote(
            part(block, c), part(block, c), fwd_send.at[(k - 1) * chunks + i],
            tok_recv.at[block * chunks + c], "tp", pair,
        )

    def arrived(block, c):
        remote(
            part(block, c), part(block, c), pair_send.at[0], tok_recv.at[block * chunks + c],
            "tp", pair,
        ).wait_recv()

    early = chunk * 3 // 128 * 16 if chunk >= 128 else chunk // 2
    for k in range(1, chips):
        across_part(k, 0, early, resid).start()
    for c in range(chunks):
        beside(c).start()

    for copy in small[:4]:
        copy.wait()
    lifted = cond[...].astype(jnp.float32)
    lifted = (lifted / (1.0 + jnp.exp(-lifted))).astype(jnp.bfloat16)
    lanes = lifted.shape[1]
    for i, m in enumerate((mshift, mscale, mgate)):
        sums = []
        for r in range(lifted.shape[0]):
            line = jnp.broadcast_to(lifted[r : r + 1, :], (16, lanes))
            sums.append(dot32(line, m[r * lanes : (r + 1) * lanes, :])[0:1])
        modsp[me_s, i : i + 1, :] = functools.reduce(jnp.add, sums)
    modsp[me_s, 3:8, :] = jnp.zeros((5, modsp.shape[2]), jnp.float32)

    def to_sp(k, buf, send, recv):
        return remote(
            buf.at[me_s], buf.at[me_s], send.at[k - 1], recv.at[me_s], "sp", lax.rem(me_s + k, sp)
        )

    def from_sp(k, buf, send, recv):
        peer = lax.rem(me_s + k, sp)
        remote(buf.at[peer], buf.at[peer], send.at[k - 1], recv.at[peer], "sp", peer).wait_recv()

    for k in range(1, sp):
        to_sp(k, modsp, msp_send, msp_recv).start()

    for copy in small[4:7]:
        copy.wait()
    load_k.wait()
    load_v.wait()
    normed = normed_tokens(context[...], gain_ref[...]).astype(jnp.bfloat16)
    own = ctxbuf.at[me_s]
    store_heads(own, 0, dot32(normed, wk[...]), kg[...])
    own[:, width:] = dot32(normed, wv[...]).astype(jnp.bfloat16)

    for copy in small[7:]:
        copy.wait()
    ob_ref[...] = jnp.zeros_like(ob_ref)
    ob_ref[:, :, : ob_in.shape[2]] = ob_in[...]

    def fill(h, carry):
        fill_bias(ob_ref, table, h)
        return carry

    lax.fori_loop(0, heads // 2, fill, 0)

    for k in range(1, sp):
        from_sp(k, modsp, msp_send, msp_recv)
    summed = modsp[0]
    for s in range(1, sp):
        summed = summed + modsp[s]
    modtp[me_t] = summed

    def to_tp(k):
        return remote(
            modtp.at[me_t], modtp.at[me_t], mtp_send.at[k - 1], mtp_recv.at[me_t], "tp",
            lax.rem(me_t + k, tp),
        )

    for k in range(1, tp):
        to_tp(k).start()
    load_tokens.wait()
    for k in range(1, chips):
        across_part(k, early, chunk - early, tok.at[me_t]).start()
    for c in range(chunks):
        arrived(pair, c)
    for i in range(1, chunks):
        for k in range(1, chips):
            across(k, i).start()

    twin = me_s + 1 - 2 * (me_s % 2)
    steps = sp // 2

    def context_copy(block, peer, index):
        return remote(
            ctxbuf.at[block], ctxbuf.at[block], ctx_send.at[index], ctx_recv.at[block], "sp", peer
        )

    def fellow(m):
        return lax.rem(me_s + 2 * (m // 2 + 1 if m % 2 == 0 else steps - m // 2 - 1), sp)

    def context_arrived(block):
        context_copy(block, twin, 0).wait_recv()

    context_copy(me_s, twin, 0).start()
    for m in range(steps - 1):
        context_copy(me_s, fellow(m), 1 + m).start()

    def pass_context(begin, end):
        for m in range(begin, end):
            context_arrived(fellow(m))
            context_copy(fellow(m), twin, steps + m).start()

    lax.fori_loop(heads // 2, heads, fill, 0)

    load_o.start()
    load_q.wait()
    for k in range(1, tp):
        peer = lax.rem(me_t + k, tp)
        remote(
            modtp.at[peer], modtp.at[peer], mtp_send.at[k - 1], mtp_recv.at[peer], "tp", peer
        ).wait_recv()
    piece = modtp.shape[2]
    for t in range(tp):
        mods[:, t * piece : (t + 1) * piece] = modtp[t]

    edge = REACH * GRID_W

    def project(block, c):
        values = tok[block, pl.ds(pl.multiple_of(c * chunk, chunk), chunk), :]
        normed = normed_tokens(values, gain_ref[...]) * (1.0 + mods[1:2, :]) + mods[0:1, :]
        normed = normed.astype(jnp.bfloat16)
        at = pl.multiple_of(block * count + c * chunk, chunk)
        store_heads(qbuf, at, dot32(normed, wq[...]), qg[...])
        at = pl.multiple_of(edge + block * count + c * chunk, GRID_W)
        store_heads(kvbuf, at, dot32(normed, wk[...]), kg[...])
        kvbuf[pl.ds(at, chunk), width:] = dot32(normed, wv[...]).astype(jnp.bfloat16)

    def local_step(c, carry):
        project(me_t, c)
        return carry

    lax.fori_loop(0, chunks, local_step, 0)
    near = min(2, steps - 1)
    pass_context(0, near)

    def pair_step(c, carry):
        project(pair, c)
        return carry

    lax.fori_loop(0, chunks, pair_step, 0)
    pass_context(near, steps - 1)

    ahead = (WIN_ROWS - REACH - 1) * GRID_W

    def up():
        return remote(
            kvbuf.at[pl.ds(edge, ahead), :], kvbuf.at[pl.ds(edge + tokens, ahead), :],
            halo_send.at[0], halo_recv.at[0], "sp", me_s - 1,
        )

    def down():
        return remote(
            kvbuf.at[pl.ds(tokens, edge), :], kvbuf.at[pl.ds(0, edge), :],
            halo_send.at[1], halo_recv.at[1], "sp", me_s + 1,
        )

    upper = chip < (chips + 1) // 2
    lower = jnp.logical_not(upper)

    def send_up(when):
        @pl.when(when & (me_s > 0))
        def _():
            up().start()

    def send_down(when):
        @pl.when(when & (me_s < sp - 1))
        def _():
            down().start()

    @pl.when(me_s == 0)
    def _():
        kvbuf[0:edge, :] = jnp.zeros((edge, 2 * width), jnp.bfloat16)

    kvbuf[edge + tokens + ahead :, :] = jnp.zeros((edge - ahead, 2 * width), jnp.bfloat16)

    @pl.when(me_s == sp - 1)
    def _():
        kvbuf[edge + tokens : edge + tokens + ahead, :] = jnp.zeros((ahead, 2 * width), jnp.bfloat16)

    ctx_count = ctxbuf.shape[0] * ctxbuf.shape[1]
    factor = HEAD_DIM ** (-0.5) * LOG2E
    span = edge
    blocks = rows // REACH
    half = 2 * GRID_W
    keys = 3 * span
    piece_rows = divisor(chunk_rows, 2) if REACH % 2 == 0 else 1
    piece = piece_rows * GRID_W
    per_dest = chunk_rows // piece_rows
    per_block = REACH // piece_rows
    bias_rows = 2 * WIN_ROWS - 1
    plain = list(range(bias_rows + 1))
    lead, trail, blank = bias_rows + 1, bias_rows + 2, bias_rows + 3

    def prepare(kb):
        at = pl.ds(pl.multiple_of(kb * span, span), span)
        vt[:, at] = kvbuf[at, width:].T

    def prepare_context():
        values = ctxbuf[:, :, width:].reshape(ctx_count, width)
        ctxvt[...] = values.T

    def tile_slot(line, side, first, last):
        r = line + REACH - 1 - 2 * side
        low, high = REACH - 1, REACH - 1 + WIN_ROWS
        inner = lead if r == low else trail if r == high else r if low < r < high else blank
        at_first = r if line >= REACH else blank
        at_last = r if line < 2 * REACH else blank
        if inner == at_first == at_last:
            return inner
        return inner + first * (at_first - inner) + last * (at_last - inner)

    def attend(b, first, last):
        at = pl.multiple_of(b * span, span)
        heads = width // HEAD_DIM

        def lanes_of(h, base):
            return slice(base + h * HEAD_DIM, base + (h + 1) * HEAD_DIM)

        def scores(h):
            queries = qbuf[pl.ds(at, span), lanes_of(h, 0)]
            slot = h % 2
            tops = [jnp.full((8, half), MASKED, jnp.float32) for _ in range(2)]
            for kb in range(3):
                part = dot_t(kvbuf[pl.ds(at + kb * span, span), lanes_of(h, 0)], queries)
                for i in range(REACH):
                    line = kb * REACH + i
                    for side in range(2):
                        spot = tile_slot(line, side, first, last)
                        if isinstance(spot, int) and spot == blank:
                            continue
                        cell = part[i * GRID_W : (i + 1) * GRID_W, side * half : (side + 1) * half]
                        cell = cell * factor + table[h, spot]
                        score[slot, line * GRID_W : (line + 1) * GRID_W, side * half : (side + 1) * half] = cell
                        tops[side] = jnp.maximum(tops[side], jnp.max(cell.reshape(-1, 8, half), axis=0))
            raw = jnp.full((8, 2 * half), -jnp.inf, jnp.float32)
            for c in range(ctx_count // span):
                ctx_key = ctxbuf[c * span // ctxbuf.shape[1] : (c + 1) * span // ctxbuf.shape[1], :, lanes_of(h, 0)]
                part = dot_t(ctx_key.reshape(span, HEAD_DIM), queries)
                score[slot, keys + c * span : keys + (c + 1) * span, :] = part
                raw = jnp.maximum(raw, jnp.max(part.reshape(-1, 8, 2 * half), axis=0))
            context_bias = cb[0:1, h : h + 1] * LOG2E
            top = jnp.maximum(jnp.concatenate(tops, axis=1), raw * factor + context_bias)
            return jnp.max(top, axis=0, keepdims=True), context_bias

        def finish_head(h, top, context_bias):
            slot = h % 2
            totals = []
            for side in range(2):
                cols = slice(side * half, (side + 1) * half)
                shift = jnp.broadcast_to(top[:, cols], (GRID_W, half))
                total = jnp.zeros((8, half), jnp.float32)
                for line in range(3 * REACH):
                    span_rows = slice(line * GRID_W, (line + 1) * GRID_W)
                    spot = tile_slot(line, side, first, last)
                    if isinstance(spot, int) and spot == blank:
                        prob[slot, span_rows, cols] = jnp.zeros((GRID_W, half), jnp.bfloat16)
                        continue
                    cell = jnp.exp2(score[slot, span_rows, cols] - shift)
                    total = total + jnp.sum(cell.reshape(-1, 8, half), axis=0)
                    prob[slot, span_rows, cols] = cell.astype(jnp.bfloat16)
                shift = shift - context_bias
                for c in range(ctx_count // GRID_W):
                    span_rows = slice(keys + c * GRID_W, keys + (c + 1) * GRID_W)
                    cell = jnp.exp2(score[slot, span_rows, cols] * factor - shift)
                    total = total + jnp.sum(cell.reshape(-1, 8, half), axis=0)
                    prob[slot, span_rows, cols] = cell.astype(jnp.bfloat16)
                totals.append(jnp.sum(total, axis=0, keepdims=True))
            out = dot32(vt[lanes_of(h, 0), pl.ds(at, keys)], prob[slot, :keys, :])
            out = out + dot32(ctxvt[lanes_of(h, 0), :], prob[slot, keys:, :])
            out = out * (1.0 / jnp.concatenate(totals, axis=1))
            att[pl.ds(at, span), lanes_of(h, 0)] = out.T.astype(jnp.bfloat16)

        state = scores(0)
        for h in range(heads):
            following = scores(h + 1) if h + 1 < heads else None
            finish_head(h, *state)
            state = following

    def hand(p):
        dest = p // per_dest
        local = p % per_dest
        src = pl.ds(pl.multiple_of(p * piece, piece), piece)
        dst = pl.ds(pl.multiple_of(local * piece, piece), piece)
        return remote(
            att.at[src, :], full.at[me_t, dst, :], att_send.at[p],
            att_recv.at[me_t * per_dest + local], "tp", dest,
        )

    def choose(index, for_upper, for_lower):
        value = 0
        for at, (a, b) in enumerate(zip(for_upper, for_lower)):
            value = value + jnp.where(index == at, jnp.where(upper, a, b), 0)
        return value

    def wait_top():
        @pl.when(me_s > 0)
        def _():
            down().wait_recv()

    def wait_bottom():
        @pl.when(me_s < sp - 1)
        def _():
            up().wait_recv()

    def attend_block(b):
        first = jnp.where((b == 0) & (me_s == 0), 1, 0)
        last = jnp.where((b == blocks - 1) & (me_s == sp - 1), 1, 0)
        outer = first + last

        @pl.when(outer == 0)
        def _():
            attend(b, 0, 0)

        @pl.when(outer > 0)
        def _():
            attend(b, first, last)

        for i in range(per_block):
            p = b * per_block + per_block - 1 - i

            @pl.when(p // per_dest != me_t)
            def _():
                hand(p).start()

    def far(k, i):
        far_chip = lax.rem(chip + k, chips)
        swap, c = plan(i, core)
        block = far_chip * 2 + (core + swap) % 2
        arrived(block, c)
        onward(k, i, block, c).start()
        project(block, c)
        swap, c = plan(i, 1 - core)
        block = far_chip * 2 + (1 - core + swap) % 2
        arrived(block, c)
        project(block, c)

    def context_ready():
        context_arrived(twin)
        for m in range(1, steps):
            context_arrived(lax.rem(twin + 2 * m, sp))
        prepare_context()

    if weave:
        send_up(upper)

        def prepare_all(for_upper, for_lower):
            for a, b in zip(for_upper, for_lower):
                prepare(jnp.where(upper, a, b))

        prepare_all((1, 2, 3), (4, 5, 6))

        def attend_step(j, carry):
            b = choose(j, (1, 5, 4, 3, 2, 0), (2, 4, 3, 1, 0, 5))

            @pl.when(b == 0)
            def _():
                wait_top()
                prepare(0)

            @pl.when(b == blocks - 1)
            def _():
                wait_bottom()
                prepare(blocks + 1)

            attend_block(b)
            return carry

        def weave_step(i, carry):
            far(1, i)
            send_down((lower & (i == 0)) | (upper & (i == 1)))
            send_up(lower & (i == 2))

            @pl.when(i == 1)
            def _():
                context_ready()
                prepare_all((5, 6), (2, 3))

            @pl.when(i == 2)
            def _():
                prepare_all((4,), (1,))

            middle = jnp.where(upper, 2, 3)
            begin = jnp.where(i == 2, middle, 0)
            end = jnp.where(i == 0, 0, jnp.where(i == 2, blocks, middle))
            lax.fori_loop(begin, end, attend_step, 0)
            return carry

        lax.fori_loop(0, chunks, weave_step, 0)
    else:
        def far_step(i, carry):
            far(1 + i // chunks, lax.rem(i, chunks))
            return carry

        def prepare_step(kb, carry):
            prepare(kb)
            return carry

        def plain_step(b, carry):
            attend_block(b)
            return carry

        lax.fori_loop(0, (chips - 1) * chunks, far_step, 0)
        send_up(me_s >= 0)
        send_down(me_s >= 0)
        context_ready()
        wait_top()
        wait_bottom()
        lax.fori_loop(0, blocks + 2, prepare_step, 0)
        lax.fori_loop(0, blocks, plain_step, 0)

    own = pl.ds(pl.multiple_of(me_t * count, count), count)
    full[me_t] = att[own, :]
    load_o.wait()

    tile = HEAD_DIM * divisor(d // HEAD_DIM, 4)

    def await_piece(peer, j):
        at = pl.ds(pl.multiple_of(j * piece, piece), piece)
        remote(
            full.at[peer, at, :], full.at[peer, at, :], att_send.at[0],
            att_recv.at[peer * per_dest + j], "tp", peer,
        ).wait_recv()

    def project_out(peer, at, lanes):
        return dot32(full[peer, at, :], wo[pl.ds(pl.multiple_of(peer * width, width), width), lanes])

    for j in range(per_dest):
        await_piece(pair, j)

    def near_column(n, carry):
        lanes = pl.ds(pl.multiple_of(n * tile, tile), tile)
        partial[:, lanes] = project_out(me_t, slice(None), lanes) + project_out(pair, slice(None), lanes)
        return carry

    lax.fori_loop(0, d // tile, near_column, 0, unroll=True)

    def far_piece(step, carry):
        j = per_dest - 1 - step
        at = pl.ds(pl.multiple_of(j * piece, piece), piece)
        peers = [
            lax.rem(chip + k, chips) * 2 + side for k in range(1, chips) for side in range(2)
        ]
        for peer in peers:
            await_piece(peer, j)

        def column(n, inner):
            lanes = pl.ds(pl.multiple_of(n * tile, tile), tile)
            result = partial[at, lanes]
            for peer in peers:
                result = result + project_out(peer, at, lanes)
            floats = tok[me_t, at, lanes].astype(jnp.float32)
            out_ref[at, lanes] = (floats + mods[2:3, lanes] * result).astype(jnp.bfloat16)
            return inner

        lax.fori_loop(0, d // tile, column, 0, unroll=True)
        return carry

    lax.fori_loop(0, per_dest, far_piece, 0)

    for c in range(chunks):
        beside(c).wait_send()
        for k in range(1, chips):
            across(k, c).wait_send()
            onward(k, c, me_t, c).wait_send()
    for k in range(1, sp):
        to_sp(k, modsp, msp_send, msp_recv).wait_send()
    context_copy(me_s, twin, 0).wait_send()
    for m in range(steps - 1):
        context_copy(me_s, twin, 1 + m).wait_send()
        context_copy(me_s, twin, steps + m).wait_send()
    for k in range(1, tp):
        to_tp(k).wait_send()

    def sent(p, carry):
        @pl.when(p // per_dest != me_t)
        def _():
            hand(p).wait_send()

        return carry

    lax.fori_loop(0, rows // piece_rows, sent, 0)

    @pl.when(me_s > 0)
    def _():
        up().wait_send()

    @pl.when(me_s < sp - 1)
    def _():
        down().wait_send()


def shards(
    resid,
    cond,
    mod_shift,
    mod_scale,
    mod_gate,
    norm_gain,
    context,
    w_query,
    w_key,
    w_value,
    query_gain,
    key_gain,
    offset_bias,
    context_bias,
    w_out,
):
    sp, tp = lax.axis_size("sp"), lax.axis_size("tp")
    count, d = resid.shape
    width = w_query.shape[1]
    heads = width // HEAD_DIM
    tokens = count * tp
    lanes = min(cond.shape[0], HEAD_DIM)
    chunk_rows = count // GRID_W
    chunks = divisor(chunk_rows, 3)
    pieces = chunk_rows // divisor(chunk_rows, 2)
    ctx_count = context.shape[0] * sp
    span = REACH * GRID_W
    chips = tp // 2
    bf, f32 = jnp.bfloat16, jnp.float32
    piece = mod_shift.shape[1]
    vmem = pl.BlockSpec(memory_space=pltpu.VMEM)
    hbm = pl.BlockSpec(memory_space=pltpu.HBM)
    sems = pltpu.SemaphoreType.DMA
    hops = max(1, (chips - 1) * chunks)
    return pl.pallas_call(
        functools.partial(layer_kernel, sp, tp, chunks),
        in_specs=[hbm] * 15,
        out_specs=vmem,
        out_shape=pltpu.VMEM((count, d), bf),
        scratch_shapes=[
            pltpu.VMEM((1, heads), f32),
            pltpu.VMEM((cond.shape[0] // lanes, lanes), bf),
            pltpu.VMEM(mod_shift.shape, bf),
            pltpu.VMEM(mod_scale.shape, bf),
            pltpu.VMEM(mod_gate.shape, bf),
            pltpu.VMEM((1, d), f32),
            pltpu.VMEM(context.shape, bf),
            pltpu.VMEM((1, HEAD_DIM), f32),
            pltpu.VMEM((1, HEAD_DIM), f32),
            pltpu.VMEM((offset_bias.shape[1], heads, offset_bias.shape[2]), f32),
            pltpu.VMEM((tp, count, d), bf),
            pltpu.VMEM((d, width), bf),
            pltpu.VMEM((d, width), bf),
            pltpu.VMEM((d, width), bf),
            pltpu.VMEM((width * tp, d), bf),
            pltpu.VMEM((tokens, width), bf),
            pltpu.VMEM((tokens + 2 * REACH * GRID_W, 2 * width), bf),
            pltpu.VMEM((sp, context.shape[0], 2 * width), bf),
            pltpu.VMEM((offset_bias.shape[1], heads, 2 * GRID_W), f32),
            pltpu.VMEM((heads, 2 * WIN_ROWS + 3, GRID_W, 2 * GRID_W), f32),
            pltpu.VMEM((sp, 8, piece), f32),
            pltpu.VMEM((tp, 8, piece), f32),
            pltpu.VMEM((8, d), f32),
            pltpu.VMEM((tokens, width), bf),
            pltpu.VMEM((tp, count, width), bf),
            pltpu.VMEM((width, tokens + 2 * span), bf),
            pltpu.VMEM((width, ctx_count), bf),
            pltpu.VMEM((2, 3 * span + ctx_count, span), f32),
            pltpu.VMEM((2, 3 * span + ctx_count, span), bf),
            pltpu.VMEM((count, d), f32),
            sems((15,)),
            sems((hops,)),
            sems((chunks,)),
            sems((hops,)),
            sems((tp * chunks,)),
            sems((sp,)),
            sems((sp,)),
            sems((tp,)),
            sems((tp,)),
            sems((sp,)),
            sems((sp,)),
            sems((2,)),
            sems((2,)),
            sems((tp * pieces,)),
            sems((tp * pieces,)),
        ],
        compiler_params=pltpu.CompilerParams(
            collective_id=0, has_side_effects=True, vmem_limit_bytes=VMEM_BYTES
        ),
        name="layer",
    )(
        context_bias[None, :], resid, cond.reshape(-1, lanes), mod_shift, mod_scale, mod_gate, norm_gain[None, :],
        context, w_query, w_key, w_value, query_gain[None, :], key_gain[None, :],
        jnp.transpose(offset_bias, (1, 0, 2)), w_out,
    )


def solution(mesh):
    in_specs = (
        P(("sp", "tp"), None),
        P("sp"),
        P("sp", "tp"),
        P("sp", "tp"),
        P("sp", "tp"),
        P(),
        P("sp", None),
        P(None, "tp"),
        P(None, "tp"),
        P(None, "tp"),
        P(),
        P(),
        P("tp", None, None),
        P("tp"),
        P(),
    )
    out_specs = P(("sp", "tp"), None)
    return jax.shard_map(shards, mesh=mesh, in_specs=in_specs, out_specs=out_specs, check_vma=False)
```

```python
import functools

import jax
import jax.numpy as jnp
from jax import lax
from jax.experimental import pallas as pl
from jax.experimental.pallas import tpu as pltpu
from jax.sharding import PartitionSpec as P

HEAD_DIM = 128
GRID_W = 64
WIN_ROWS = 8
WIN_COLS = 16
REACH = WIN_ROWS // 2
EPS = 1e-06
LOG2E = 1.4426950408889634
MASKED = -1e30
VMEM_BYTES = 56 * 1024 * 1024


def dot32(a, b):
    return jnp.dot(a, b, preferred_element_type=jnp.float32)


def dot_t(a, b):
    return lax.dot_general(a, b, (((1,), (1,)), ((), ())), preferred_element_type=jnp.float32)


def divisor(count, most):
    return max(d for d in range(1, most + 1) if count % d == 0)


def normed_tokens(rows, gain):
    floats = rows.astype(jnp.float32)
    inverse = lax.rsqrt(jnp.mean(floats * floats, axis=-1, keepdims=True) + EPS)
    return floats * inverse * gain


def store_heads(out_ref, at, values, gain):
    count = values.shape[0]
    for h in range(values.shape[1] // HEAD_DIM):
        part = values[:, h * HEAD_DIM : (h + 1) * HEAD_DIM]
        part = part * lax.rsqrt(jnp.mean(part * part, axis=-1, keepdims=True) + EPS) * gain
        out_ref[pl.ds(at, count), h * HEAD_DIM : (h + 1) * HEAD_DIM] = part.astype(jnp.bfloat16)


def fill_bias(ob_ref, table, h):
    rows = 2 * WIN_ROWS - 1
    lanes = 2 * GRID_W
    lane = lax.broadcasted_iota(jnp.int32, (lanes, lanes), 1)
    line = lax.broadcasted_iota(jnp.int32, (lanes, lanes), 0)
    query = line % GRID_W
    begin = jnp.clip(query - WIN_COLS // 2, 0, GRID_W - WIN_COLS)
    valid = (lane >= begin) & (lane < begin + WIN_COLS)

    def spread(r):
        row = jnp.broadcast_to(ob_ref[r, pl.ds(h, 1), :], (GRID_W, lanes))
        return pltpu.roll(row, lanes - (WIN_COLS - 1), 1, stride=1, stride_axis=0)

    masked = jnp.full((GRID_W, lanes), MASKED, jnp.float32)

    def put(slot, first, second):
        both = jnp.concatenate([first, second], axis=0) * LOG2E
        both = jnp.where(valid, both, MASKED)
        table[h, slot] = both.T[:GRID_W]

    low, high = REACH - 1, REACH - 1 + WIN_ROWS
    spreads = [spread(r) for r in range(rows)]
    for r in range(rows + 1):
        put(r, spreads[r] if r < rows else masked, spreads[r - 1] if r > 0 else masked)
    put(rows + 1, spreads[low], masked)
    put(rows + 2, masked, spreads[high - 1])
    table[h, rows + 3] = masked


def layer_kernel(
    sp, tp, chunks, cb_hbm, resid, cond_hbm, mshift_hbm, mscale_hbm, mgate_hbm, gain_hbm, context_hbm,
    wq_hbm, wk_hbm, wv_hbm, qg_hbm, kg_hbm, ob_hbm, wo_hbm, out_ref,
    cb, cond, mshift, mscale, mgate, gain_ref, context, qg, kg, ob_in,
    tok, wq, wk, wv, wo, qbuf, kvbuf, ctxbuf, ob_ref, table, modsp, modtp, mods, att, full,
    vt, ctxvt, score, prob, partial,
    load_sem, tok_send, pair_send, fwd_send, tok_recv, msp_send, msp_recv, mtp_send, mtp_recv,
    ctx_send, ctx_recv, halo_send, halo_recv, att_send, att_recv,
):
    me_s, me_t = lax.axis_index("sp"), lax.axis_index("tp")
    count, d = resid.shape
    chunk = count // chunks
    width = wq.shape[1]
    heads = width // HEAD_DIM
    tokens = count * tp
    rows = tokens // GRID_W
    total_rows = rows * sp
    first = me_s * rows
    chips = tp // 2
    chip, core = me_t // 2, me_t % 2
    pair = chip * 2 + (1 - core)

    def remote(src, dst, send, recv, axis, peer):
        return pltpu.make_async_remote_copy(
            src_ref=src, dst_ref=dst, send_sem=send, recv_sem=recv,
            device_id={axis: peer}, device_id_type=pl.DeviceIdType.MESH,
        )

    barrier = pltpu.get_barrier_semaphore()
    for k in range(1, sp):
        pl.semaphore_signal(
            barrier, inc=1, device_id={"sp": lax.rem(me_s + k, sp)},
            device_id_type=pl.DeviceIdType.MESH,
        )
    for k in range(1, tp):
        pl.semaphore_signal(
            barrier, inc=1, device_id={"tp": lax.rem(me_t + k, tp)},
            device_id_type=pl.DeviceIdType.MESH,
        )

    def load(index, src, dst):
        return pltpu.make_async_copy(src, dst, load_sem.at[index])

    small = [
        load(i, src, dst)
        for i, (src, dst) in enumerate(
            (
                (cond_hbm, cond), (mshift_hbm, mshift), (mscale_hbm, mscale), (mgate_hbm, mgate),
                (context_hbm, context), (gain_hbm, gain_ref), (kg_hbm, kg), (qg_hbm, qg),
                (ob_hbm, ob_in), (cb_hbm, cb),
            )
        )
    ]
    base = len(small)
    load_k, load_v = load(base, wk_hbm, wk), load(base + 1, wv_hbm, wv)
    load_q, load_o = load(base + 2, wq_hbm, wq), load(base + 3, wo_hbm, wo)
    load_tokens = load(base + 4, resid, tok.at[me_t])
    for copy in small[:6] + [load_tokens, load_k, load_v] + small[6:] + [load_q]:
        copy.start()
    pl.semaphore_wait(barrier, sp + tp - 2)

    def part(block, c):
        return tok.at[block, pl.ds(pl.multiple_of(c * chunk, chunk), chunk), :]

    def mine(c):
        return resid.at[pl.ds(pl.multiple_of(c * chunk, chunk), chunk), :]

    chunk_rows = rows // tp
    weave = chips == 2 and chunks == 3 and chunk_rows == 6

    def plan(i, side):
        if not weave:
            return 0, i
        return jnp.where(i == 1 + side, 1, 0), jnp.where(i == 0, chunks - 1, side)

    def across(k, i):
        peer = lax.rem(chip + k, chips) * 2 + core
        swap, c = plan(i, core)
        owner = chip * 2 + (core + swap) % 2
        return remote(
            part(owner, c), part(owner, c), tok_send.at[(k - 1) * chunks + i],
            tok_recv.at[owner * chunks + c], "tp", peer,
        )

    def across_part(k, begin, size, src):
        peer = lax.rem(chip + k, chips) * 2 + core
        c = plan(0, core)[1]
        at = pl.ds(pl.multiple_of(c * chunk + begin, 16), size)
        return remote(
            src.at[at, :], tok.at[me_t, at, :], tok_send.at[(k - 1) * chunks],
            tok_recv.at[me_t * chunks + c], "tp", peer,
        )

    def beside(c):
        return remote(
            mine(c), part(me_t, c), pair_send.at[c], tok_recv.at[me_t * chunks + c], "tp", pair
        )

    def onward(k, i, block, c):
        return remote(
            part(block, c), part(block, c), fwd_send.at[(k - 1) * chunks + i],
            tok_recv.at[block * chunks + c], "tp", pair,
        )

    def arrived(block, c):
        remote(
            part(block, c), part(block, c), pair_send.at[0], tok_recv.at[block * chunks + c],
            "tp", pair,
        ).wait_recv()

    early = chunk * 3 // 128 * 16 if chunk >= 128 else chunk // 2
    for k in range(1, chips):
        across_part(k, 0, early, resid).start()
    for c in range(chunks):
        beside(c).start()

    for copy in small[:4]:
        copy.wait()
    lifted = cond[...].astype(jnp.float32)
    lifted = (lifted / (1.0 + jnp.exp(-lifted))).astype(jnp.bfloat16)
    lanes = lifted.shape[1]
    for i, m in enumerate((mshift, mscale, mgate)):
        sums = []
        for r in range(lifted.shape[0]):
            line = jnp.broadcast_to(lifted[r : r + 1, :], (16, lanes))
            sums.append(dot32(line, m[r * lanes : (r + 1) * lanes, :])[0:1])
        modsp[me_s, i : i + 1, :] = functools.reduce(jnp.add, sums)
    modsp[me_s, 3:8, :] = jnp.zeros((5, modsp.shape[2]), jnp.float32)

    def to_sp(k, buf, send, recv):
        return remote(
            buf.at[me_s], buf.at[me_s], send.at[k - 1], recv.at[me_s], "sp", lax.rem(me_s + k, sp)
        )

    def from_sp(k, buf, send, recv):
        peer = lax.rem(me_s + k, sp)
        remote(buf.at[peer], buf.at[peer], send.at[k - 1], recv.at[peer], "sp", peer).wait_recv()

    for k in range(1, sp):
        to_sp(k, modsp, msp_send, msp_recv).start()

    for copy in small[4:7]:
        copy.wait()
    load_k.wait()
    load_v.wait()
    normed = normed_tokens(context[...], gain_ref[...]).astype(jnp.bfloat16)
    own = ctxbuf.at[me_s]
    store_heads(own, 0, dot32(normed, wk[...]), kg[...])
    own[:, width:] = dot32(normed, wv[...]).astype(jnp.bfloat16)

    for copy in small[7:]:
        copy.wait()
    ob_ref[...] = jnp.zeros_like(ob_ref)
    ob_ref[:, :, : ob_in.shape[2]] = ob_in[...]

    def fill(h, carry):
        fill_bias(ob_ref, table, h)
        return carry

    lax.fori_loop(0, heads // 2, fill, 0)

    for k in range(1, sp):
        from_sp(k, modsp, msp_send, msp_recv)
    summed = modsp[0]
    for s in range(1, sp):
        summed = summed + modsp[s]
    modtp[me_t] = summed

    def to_tp(k):
        return remote(
            modtp.at[me_t], modtp.at[me_t], mtp_send.at[k - 1], mtp_recv.at[me_t], "tp",
            lax.rem(me_t + k, tp),
        )

    for k in range(1, tp):
        to_tp(k).start()
    load_tokens.wait()
    for k in range(1, chips):
        across_part(k, early, chunk - early, tok.at[me_t]).start()
    for c in range(chunks):
        arrived(pair, c)
    for i in range(1, chunks):
        for k in range(1, chips):
            across(k, i).start()

    twin = me_s + 1 - 2 * (me_s % 2)
    steps = sp // 2

    def context_copy(block, peer, index):
        return remote(
            ctxbuf.at[block], ctxbuf.at[block], ctx_send.at[index], ctx_recv.at[block], "sp", peer
        )

    def fellow(m):
        return lax.rem(me_s + 2 * (m // 2 + 1 if m % 2 == 0 else steps - m // 2 - 1), sp)

    def context_arrived(block):
        context_copy(block, twin, 0).wait_recv()

    context_copy(me_s, twin, 0).start()
    for m in range(steps - 1):
        context_copy(me_s, fellow(m), 1 + m).start()

    def pass_context(begin, end):
        for m in range(begin, end):
            context_arrived(fellow(m))
            context_copy(fellow(m), twin, steps + m).start()

    lax.fori_loop(heads // 2, heads, fill, 0)

    load_o.start()
    load_q.wait()
    for k in range(1, tp):
        peer = lax.rem(me_t + k, tp)
        remote(
            modtp.at[peer], modtp.at[peer], mtp_send.at[k - 1], mtp_recv.at[peer], "tp", peer
        ).wait_recv()
    piece = modtp.shape[2]
    for t in range(tp):
        mods[:, t * piece : (t + 1) * piece] = modtp[t]

    edge = REACH * GRID_W

    def project(block, c):
        values = tok[block, pl.ds(pl.multiple_of(c * chunk, chunk), chunk), :]
        normed = normed_tokens(values, gain_ref[...]) * (1.0 + mods[1:2, :]) + mods[0:1, :]
        normed = normed.astype(jnp.bfloat16)
        at = pl.multiple_of(block * count + c * chunk, chunk)
        store_heads(qbuf, at, dot32(normed, wq[...]), qg[...])
        at = pl.multiple_of(edge + block * count + c * chunk, GRID_W)
        store_heads(kvbuf, at, dot32(normed, wk[...]), kg[...])
        kvbuf[pl.ds(at, chunk), width:] = dot32(normed, wv[...]).astype(jnp.bfloat16)

    def local_step(c, carry):
        project(me_t, c)
        return carry

    lax.fori_loop(0, chunks, local_step, 0)
    near = min(2, steps - 1)
    pass_context(0, near)

    def pair_step(c, carry):
        project(pair, c)
        return carry

    lax.fori_loop(0, chunks, pair_step, 0)
    pass_context(near, steps - 1)

    ahead = (WIN_ROWS - REACH - 1) * GRID_W

    def up():
        return remote(
            kvbuf.at[pl.ds(edge, ahead), :], kvbuf.at[pl.ds(edge + tokens, ahead), :],
            halo_send.at[0], halo_recv.at[0], "sp", me_s - 1,
        )

    def down():
        return remote(
            kvbuf.at[pl.ds(tokens, edge), :], kvbuf.at[pl.ds(0, edge), :],
            halo_send.at[1], halo_recv.at[1], "sp", me_s + 1,
        )

    upper = chip < (chips + 1) // 2
    lower = jnp.logical_not(upper)

    def send_up(when):
        @pl.when(when & (me_s > 0))
        def _():
            up().start()

    def send_down(when):
        @pl.when(when & (me_s < sp - 1))
        def _():
            down().start()

    @pl.when(me_s == 0)
    def _():
        kvbuf[0:edge, :] = jnp.zeros((edge, 2 * width), jnp.bfloat16)

    kvbuf[edge + tokens + ahead :, :] = jnp.zeros((edge - ahead, 2 * width), jnp.bfloat16)

    @pl.when(me_s == sp - 1)
    def _():
        kvbuf[edge + tokens : edge + tokens + ahead, :] = jnp.zeros((ahead, 2 * width), jnp.bfloat16)

    ctx_count = ctxbuf.shape[0] * ctxbuf.shape[1]
    factor = HEAD_DIM ** (-0.5) * LOG2E
    span = edge
    blocks = rows // REACH
    half = 2 * GRID_W
    keys = 3 * span
    piece_rows = divisor(chunk_rows, 2) if REACH % 2 == 0 else 1
    piece = piece_rows * GRID_W
    per_dest = chunk_rows // piece_rows
    per_block = REACH // piece_rows
    bias_rows = 2 * WIN_ROWS - 1
    plain = list(range(bias_rows + 1))
    lead, trail, blank = bias_rows + 1, bias_rows + 2, bias_rows + 3

    def prepare(kb):
        at = pl.ds(pl.multiple_of(kb * span, span), span)
        vt[:, at] = kvbuf[at, width:].T

    def prepare_context():
        values = ctxbuf[:, :, width:].reshape(ctx_count, width)
        ctxvt[...] = values.T

    def tile_slot(line, side, first, last):
        r = line + REACH - 1 - 2 * side
        low, high = REACH - 1, REACH - 1 + WIN_ROWS
        inner = lead if r == low else trail if r == high else r if low < r < high else blank
        at_first = r if line >= REACH else blank
        at_last = r if line < 2 * REACH else blank
        if inner == at_first == at_last:
            return inner
        return inner + first * (at_first - inner) + last * (at_last - inner)

    def attend(b, first, last):
        at = pl.multiple_of(b * span, span)
        heads = width // HEAD_DIM

        def lanes_of(h, base):
            return slice(base + h * HEAD_DIM, base + (h + 1) * HEAD_DIM)

        def scores(h):
            queries = qbuf[pl.ds(at, span), lanes_of(h, 0)]
            slot = h % 2
            tops = [jnp.full((8, half), MASKED, jnp.float32) for _ in range(2)]
            for kb in range(3):
                part = dot_t(kvbuf[pl.ds(at + kb * span, span), lanes_of(h, 0)], queries)
                for i in range(REACH):
                    line = kb * REACH + i
                    for side in range(2):
                        spot = tile_slot(line, side, first, last)
                        if isinstance(spot, int) and spot == blank:
                            continue
                        cell = part[i * GRID_W : (i + 1) * GRID_W, side * half : (side + 1) * half]
                        cell = cell * factor + table[h, spot]
                        score[slot, line * GRID_W : (line + 1) * GRID_W, side * half : (side + 1) * half] = cell
                        tops[side] = jnp.maximum(tops[side], jnp.max(cell.reshape(-1, 8, half), axis=0))
            raw = jnp.full((8, 2 * half), -jnp.inf, jnp.float32)
            for c in range(ctx_count // span):
                ctx_key = ctxbuf[c * span // ctxbuf.shape[1] : (c + 1) * span // ctxbuf.shape[1], :, lanes_of(h, 0)]
                part = dot_t(ctx_key.reshape(span, HEAD_DIM), queries)
                score[slot, keys + c * span : keys + (c + 1) * span, :] = part
                raw = jnp.maximum(raw, jnp.max(part.reshape(-1, 8, 2 * half), axis=0))
            context_bias = cb[0:1, h : h + 1] * LOG2E
            top = jnp.maximum(jnp.concatenate(tops, axis=1), raw * factor + context_bias)
            return jnp.max(top, axis=0, keepdims=True), context_bias

        def finish_head(h, top, context_bias):
            slot = h % 2
            totals = []
            for side in range(2):
                cols = slice(side * half, (side + 1) * half)
                shift = jnp.broadcast_to(top[:, cols], (GRID_W, half))
                total = jnp.zeros((8, half), jnp.float32)
                for line in range(3 * REACH):
                    span_rows = slice(line * GRID_W, (line + 1) * GRID_W)
                    spot = tile_slot(line, side, first, last)
                    if isinstance(spot, int) and spot == blank:
                        prob[slot, span_rows, cols] = jnp.zeros((GRID_W, half), jnp.bfloat16)
                        continue
                    cell = jnp.exp2(score[slot, span_rows, cols] - shift)
                    total = total + jnp.sum(cell.reshape(-1, 8, half), axis=0)
                    prob[slot, span_rows, cols] = cell.astype(jnp.bfloat16)
                shift = shift - context_bias
                for c in range(ctx_count // GRID_W):
                    span_rows = slice(keys + c * GRID_W, keys + (c + 1) * GRID_W)
                    cell = jnp.exp2(score[slot, span_rows, cols] * factor - shift)
                    total = total + jnp.sum(cell.reshape(-1, 8, half), axis=0)
                    prob[slot, span_rows, cols] = cell.astype(jnp.bfloat16)
                totals.append(jnp.sum(total, axis=0, keepdims=True))
            out = dot32(vt[lanes_of(h, 0), pl.ds(at, keys)], prob[slot, :keys, :])
            out = out + dot32(ctxvt[lanes_of(h, 0), :], prob[slot, keys:, :])
            out = out * (1.0 / jnp.concatenate(totals, axis=1))
            att[pl.ds(at, span), lanes_of(h, 0)] = out.T.astype(jnp.bfloat16)

        state = scores(0)
        for h in range(heads):
            following = scores(h + 1) if h + 1 < heads else None
            finish_head(h, *state)
            state = following

    def hand(p):
        dest = p // per_dest
        local = p % per_dest
        src = pl.ds(pl.multiple_of(p * piece, piece), piece)
        dst = pl.ds(pl.multiple_of(local * piece, piece), piece)
        return remote(
            att.at[src, :], full.at[me_t, dst, :], att_send.at[p],
            att_recv.at[me_t * per_dest + local], "tp", dest,
        )

    def choose(index, for_upper, for_lower):
        value = 0
        for at, (a, b) in enumerate(zip(for_upper, for_lower)):
            value = value + jnp.where(index == at, jnp.where(upper, a, b), 0)
        return value

    def wait_top():
        @pl.when(me_s > 0)
        def _():
            down().wait_recv()

    def wait_bottom():
        @pl.when(me_s < sp - 1)
        def _():
            up().wait_recv()

    def attend_block(b):
        first = jnp.where((b == 0) & (me_s == 0), 1, 0)
        last = jnp.where((b == blocks - 1) & (me_s == sp - 1), 1, 0)
        outer = first + last

        @pl.when(outer == 0)
        def _():
            attend(b, 0, 0)

        @pl.when(outer > 0)
        def _():
            attend(b, first, last)

    def hand_block(b):
        for i in range(per_block):
            p = b * per_block + per_block - 1 - i

            @pl.when(p // per_dest != me_t)
            def _():
                hand(p).start()

    def far(k, i, on_arrival=None):
        far_chip = lax.rem(chip + k, chips)
        swap, c = plan(i, core)
        block = far_chip * 2 + (core + swap) % 2
        arrived(block, c)
        onward(k, i, block, c).start()
        if on_arrival is not None:
            on_arrival()
        project(block, c)
        swap, c = plan(i, 1 - core)
        block = far_chip * 2 + (1 - core + swap) % 2
        arrived(block, c)
        project(block, c)

    def context_ready():
        context_arrived(twin)
        for m in range(1, steps):
            context_arrived(lax.rem(twin + 2 * m, sp))
        prepare_context()

    if weave:
        send_up(upper)

        def prepare_all(for_upper, for_lower):
            for a, b in zip(for_upper, for_lower):
                prepare(jnp.where(upper, a, b))

        prepare_all((1, 2, 3), (4, 5, 6))

        def attend_step(j, carry):
            b = choose(j, (1, 5, 4, 3, 2, 0), (4, 2, 1, 0, 3, 5))

            @pl.when(b == 0)
            def _():
                wait_top()
                prepare(0)

            @pl.when(b == blocks - 1)
            def _():
                wait_bottom()
                prepare(blocks + 1)

            attend_block(b)

            @pl.when(b != early_block)
            def _():
                hand_block(b)

            return carry

        early_block = jnp.where(upper, 5, 2)

        def weave_step(i, carry):
            def hand_early():
                @pl.when(i == 2)
                def _():
                    hand_block(early_block)

            far(1, i, hand_early)
            send_down((lower & (i == 0)) | (upper & (i == 1)))
            send_up(lower & (i == 2))

            @pl.when(i == 1)
            def _():
                context_ready()
                prepare_all((5, 6), (2, 3))

            @pl.when(i == 2)
            def _():
                prepare_all((4,), (1,))

            begin = jnp.where(i == 2, 2, 0)
            end = jnp.where(i == 0, 0, jnp.where(i == 2, blocks, 2))
            lax.fori_loop(begin, end, attend_step, 0)
            return carry

        lax.fori_loop(0, chunks, weave_step, 0)
    else:
        def far_step(i, carry):
            far(1 + i // chunks, lax.rem(i, chunks))
            return carry

        def prepare_step(kb, carry):
            prepare(kb)
            return carry

        def plain_step(b, carry):
            attend_block(b)
            hand_block(b)
            return carry

        lax.fori_loop(0, (chips - 1) * chunks, far_step, 0)
        send_up(me_s >= 0)
        send_down(me_s >= 0)
        context_ready()
        wait_top()
        wait_bottom()
        lax.fori_loop(0, blocks + 2, prepare_step, 0)
        lax.fori_loop(0, blocks, plain_step, 0)

    own = pl.ds(pl.multiple_of(me_t * count, count), count)
    full[me_t] = att[own, :]
    load_o.wait()

    tile = HEAD_DIM * divisor(d // HEAD_DIM, 4)

    def await_piece(peer, j):
        at = pl.ds(pl.multiple_of(j * piece, piece), piece)
        remote(
            full.at[peer, at, :], full.at[peer, at, :], att_send.at[0],
            att_recv.at[peer * per_dest + j], "tp", peer,
        ).wait_recv()

    def project_out(peer, at, lanes):
        return dot32(full[peer, at, :], wo[pl.ds(pl.multiple_of(peer * width, width), width), lanes])

    for j in range(per_dest):
        await_piece(pair, j)

    def near_column(n, carry):
        lanes = pl.ds(pl.multiple_of(n * tile, tile), tile)
        partial[:, lanes] = project_out(me_t, slice(None), lanes) + project_out(pair, slice(None), lanes)
        return carry

    lax.fori_loop(0, d // tile, near_column, 0, unroll=True)

    def far_piece(step, carry):
        j = per_dest - 1 - step
        at = pl.ds(pl.multiple_of(j * piece, piece), piece)
        peers = [
            lax.rem(chip + k, chips) * 2 + side for k in range(1, chips) for side in range(2)
        ]
        for peer in peers:
            await_piece(peer, j)

        def column(n, inner):
            lanes = pl.ds(pl.multiple_of(n * tile, tile), tile)
            result = partial[at, lanes]
            for peer in peers:
                result = result + project_out(peer, at, lanes)
            floats = tok[me_t, at, lanes].astype(jnp.float32)
            out_ref[at, lanes] = (floats + mods[2:3, lanes] * result).astype(jnp.bfloat16)
            return inner

        lax.fori_loop(0, d // tile, column, 0, unroll=True)
        return carry

    lax.fori_loop(0, per_dest, far_piece, 0)

    for c in range(chunks):
        beside(c).wait_send()
        for k in range(1, chips):
            across(k, c).wait_send()
            onward(k, c, me_t, c).wait_send()
    for k in range(1, sp):
        to_sp(k, modsp, msp_send, msp_recv).wait_send()
    context_copy(me_s, twin, 0).wait_send()
    for m in range(steps - 1):
        context_copy(me_s, twin, 1 + m).wait_send()
        context_copy(me_s, twin, steps + m).wait_send()
    for k in range(1, tp):
        to_tp(k).wait_send()

    def sent(p, carry):
        @pl.when(p // per_dest != me_t)
        def _():
            hand(p).wait_send()

        return carry

    lax.fori_loop(0, rows // piece_rows, sent, 0)

    @pl.when(me_s > 0)
    def _():
        up().wait_send()

    @pl.when(me_s < sp - 1)
    def _():
        down().wait_send()


def shards(
    resid,
    cond,
    mod_shift,
    mod_scale,
    mod_gate,
    norm_gain,
    context,
    w_query,
    w_key,
    w_value,
    query_gain,
    key_gain,
    offset_bias,
    context_bias,
    w_out,
):
    sp, tp = lax.axis_size("sp"), lax.axis_size("tp")
    count, d = resid.shape
    width = w_query.shape[1]
    heads = width // HEAD_DIM
    tokens = count * tp
    lanes = min(cond.shape[0], HEAD_DIM)
    chunk_rows = count // GRID_W
    chunks = divisor(chunk_rows, 3)
    pieces = chunk_rows // divisor(chunk_rows, 2)
    ctx_count = context.shape[0] * sp
    span = REACH * GRID_W
    chips = tp // 2
    bf, f32 = jnp.bfloat16, jnp.float32
    piece = mod_shift.shape[1]
    vmem = pl.BlockSpec(memory_space=pltpu.VMEM)
    hbm = pl.BlockSpec(memory_space=pltpu.HBM)
    sems = pltpu.SemaphoreType.DMA
    hops = max(1, (chips - 1) * chunks)
    return pl.pallas_call(
        functools.partial(layer_kernel, sp, tp, chunks),
        in_specs=[hbm] * 15,
        out_specs=vmem,
        out_shape=pltpu.VMEM((count, d), bf),
        scratch_shapes=[
            pltpu.VMEM((1, heads), f32),
            pltpu.VMEM((cond.shape[0] // lanes, lanes), bf),
            pltpu.VMEM(mod_shift.shape, bf),
            pltpu.VMEM(mod_scale.shape, bf),
            pltpu.VMEM(mod_gate.shape, bf),
            pltpu.VMEM((1, d), f32),
            pltpu.VMEM(context.shape, bf),
            pltpu.VMEM((1, HEAD_DIM), f32),
            pltpu.VMEM((1, HEAD_DIM), f32),
            pltpu.VMEM((offset_bias.shape[1], heads, offset_bias.shape[2]), f32),
            pltpu.VMEM((tp, count, d), bf),
            pltpu.VMEM((d, width), bf),
            pltpu.VMEM((d, width), bf),
            pltpu.VMEM((d, width), bf),
            pltpu.VMEM((width * tp, d), bf),
            pltpu.VMEM((tokens, width), bf),
            pltpu.VMEM((tokens + 2 * REACH * GRID_W, 2 * width), bf),
            pltpu.VMEM((sp, context.shape[0], 2 * width), bf),
            pltpu.VMEM((offset_bias.shape[1], heads, 2 * GRID_W), f32),
            pltpu.VMEM((heads, 2 * WIN_ROWS + 3, GRID_W, 2 * GRID_W), f32),
            pltpu.VMEM((sp, 8, piece), f32),
            pltpu.VMEM((tp, 8, piece), f32),
            pltpu.VMEM((8, d), f32),
            pltpu.VMEM((tokens, width), bf),
            pltpu.VMEM((tp, count, width), bf),
            pltpu.VMEM((width, tokens + 2 * span), bf),
            pltpu.VMEM((width, ctx_count), bf),
            pltpu.VMEM((2, 3 * span + ctx_count, span), f32),
            pltpu.VMEM((2, 3 * span + ctx_count, span), bf),
            pltpu.VMEM((count, d), f32),
            sems((15,)),
            sems((hops,)),
            sems((chunks,)),
            sems((hops,)),
            sems((tp * chunks,)),
            sems((sp,)),
            sems((sp,)),
            sems((tp,)),
            sems((tp,)),
            sems((sp,)),
            sems((sp,)),
            sems((2,)),
            sems((2,)),
            sems((tp * pieces,)),
            sems((tp * pieces,)),
        ],
        compiler_params=pltpu.CompilerParams(
            collective_id=0, has_side_effects=True, vmem_limit_bytes=VMEM_BYTES
        ),
        name="layer",
    )(
        context_bias[None, :], resid, cond.reshape(-1, lanes), mod_shift, mod_scale, mod_gate, norm_gain[None, :],
        context, w_query, w_key, w_value, query_gain[None, :], key_gain[None, :],
        jnp.transpose(offset_bias, (1, 0, 2)), w_out,
    )


def solution(mesh):
    in_specs = (
        P(("sp", "tp"), None),
        P("sp"),
        P("sp", "tp"),
        P("sp", "tp"),
        P("sp", "tp"),
        P(),
        P("sp", None),
        P(None, "tp"),
        P(None, "tp"),
        P(None, "tp"),
        P(),
        P(),
        P("tp", None, None),
        P("tp"),
        P(),
    )
    out_specs = P(("sp", "tp"), None)
    return jax.shard_map(shards, mesh=mesh, in_specs=in_specs, out_specs=out_specs, check_vma=False)
```

```python
import functools

import jax
import jax.numpy as jnp
from jax import lax
from jax.experimental import pallas as pl
from jax.experimental.pallas import tpu as pltpu
from jax.sharding import PartitionSpec as P

HEAD_DIM = 128
GRID_W = 64
WIN_ROWS = 8
WIN_COLS = 16
REACH = WIN_ROWS // 2
EPS = 1e-06
LOG2E = 1.4426950408889634
MASKED = -1e30
VMEM_BYTES = 56 * 1024 * 1024


def dot32(a, b):
    return jnp.dot(a, b, preferred_element_type=jnp.float32)


def dot_t(a, b):
    return lax.dot_general(a, b, (((1,), (1,)), ((), ())), preferred_element_type=jnp.float32)


def divisor(count, most):
    return max(d for d in range(1, most + 1) if count % d == 0)


def normed_tokens(rows, gain):
    floats = rows.astype(jnp.float32)
    inverse = lax.rsqrt(jnp.mean(floats * floats, axis=-1, keepdims=True) + EPS)
    return floats * inverse * gain


def store_heads(out_ref, at, values, gain):
    count = values.shape[0]
    for h in range(values.shape[1] // HEAD_DIM):
        part = values[:, h * HEAD_DIM : (h + 1) * HEAD_DIM]
        part = part * lax.rsqrt(jnp.mean(part * part, axis=-1, keepdims=True) + EPS) * gain
        out_ref[pl.ds(at, count), h * HEAD_DIM : (h + 1) * HEAD_DIM] = part.astype(jnp.bfloat16)


def fill_bias(ob_ref, table, h):
    rows = 2 * WIN_ROWS - 1
    lanes = 2 * GRID_W
    lane = lax.broadcasted_iota(jnp.int32, (lanes, lanes), 1)
    line = lax.broadcasted_iota(jnp.int32, (lanes, lanes), 0)
    query = line % GRID_W
    begin = jnp.clip(query - WIN_COLS // 2, 0, GRID_W - WIN_COLS)
    valid = (lane >= begin) & (lane < begin + WIN_COLS)

    def spread(r):
        row = jnp.broadcast_to(ob_ref[r, pl.ds(h, 1), :], (GRID_W, lanes))
        return pltpu.roll(row, lanes - (WIN_COLS - 1), 1, stride=1, stride_axis=0)

    masked = jnp.full((GRID_W, lanes), MASKED, jnp.float32)

    def put(slot, first, second):
        both = jnp.concatenate([first, second], axis=0) * LOG2E
        both = jnp.where(valid, both, MASKED)
        table[h, slot] = both.T[:GRID_W]

    low, high = REACH - 1, REACH - 1 + WIN_ROWS
    spreads = [spread(r) for r in range(rows)]
    for r in range(rows + 1):
        put(r, spreads[r] if r < rows else masked, spreads[r - 1] if r > 0 else masked)
    put(rows + 1, spreads[low], masked)
    put(rows + 2, masked, spreads[high - 1])
    table[h, rows + 3] = masked


def layer_kernel(
    sp, tp, chunks, cb_hbm, resid, cond_hbm, mshift_hbm, mscale_hbm, mgate_hbm, gain_hbm, context_hbm,
    wq_hbm, wk_hbm, wv_hbm, qg_hbm, kg_hbm, ob_hbm, wo_hbm, out_ref,
    cb, cond, mshift, mscale, mgate, gain_ref, context, qg, kg, ob_in,
    tok, wq, wk, wv, wo, qbuf, kvbuf, ctxbuf, ob_ref, table, modsp, modtp, mods, att, full,
    vt, ctxvt, score, prob, partial,
    load_sem, tok_send, pair_send, fwd_send, tok_recv, msp_send, msp_recv, mtp_send, mtp_recv,
    ctx_send, ctx_recv, halo_send, halo_recv, att_send, att_recv,
):
    me_s, me_t = lax.axis_index("sp"), lax.axis_index("tp")
    count, d = resid.shape
    chunk = count // chunks
    width = wq.shape[1]
    heads = width // HEAD_DIM
    tokens = count * tp
    rows = tokens // GRID_W
    total_rows = rows * sp
    first = me_s * rows
    chips = tp // 2
    chip, core = me_t // 2, me_t % 2
    pair = chip * 2 + (1 - core)

    def remote(src, dst, send, recv, axis, peer):
        return pltpu.make_async_remote_copy(
            src_ref=src, dst_ref=dst, send_sem=send, recv_sem=recv,
            device_id={axis: peer}, device_id_type=pl.DeviceIdType.MESH,
        )

    barrier = pltpu.get_barrier_semaphore()
    for k in range(1, sp):
        pl.semaphore_signal(
            barrier, inc=1, device_id={"sp": lax.rem(me_s + k, sp)},
            device_id_type=pl.DeviceIdType.MESH,
        )
    for k in range(1, tp):
        pl.semaphore_signal(
            barrier, inc=1, device_id={"tp": lax.rem(me_t + k, tp)},
            device_id_type=pl.DeviceIdType.MESH,
        )

    def load(index, src, dst):
        return pltpu.make_async_copy(src, dst, load_sem.at[index])

    small = [
        load(i, src, dst)
        for i, (src, dst) in enumerate(
            (
                (cond_hbm, cond), (mshift_hbm, mshift), (mscale_hbm, mscale), (mgate_hbm, mgate),
                (context_hbm, context), (gain_hbm, gain_ref), (kg_hbm, kg), (qg_hbm, qg),
                (ob_hbm, ob_in), (cb_hbm, cb),
            )
        )
    ]
    base = len(small)
    load_k, load_v = load(base, wk_hbm, wk), load(base + 1, wv_hbm, wv)
    load_q, load_o = load(base + 2, wq_hbm, wq), load(base + 3, wo_hbm, wo)
    load_tokens = load(base + 4, resid, tok.at[me_t])
    for copy in small[:6] + [load_tokens, load_k, load_v] + small[6:] + [load_q]:
        copy.start()
    pl.semaphore_wait(barrier, sp + tp - 2)

    def part(block, c):
        return tok.at[block, pl.ds(pl.multiple_of(c * chunk, chunk), chunk), :]

    def mine(c):
        return resid.at[pl.ds(pl.multiple_of(c * chunk, chunk), chunk), :]

    chunk_rows = rows // tp
    weave = chips == 2 and chunks == 3 and chunk_rows == 6

    def plan(i, side):
        if not weave:
            return 0, i
        return jnp.where(i == 1 + side, 1, 0), jnp.where(i == 0, chunks - 1, side)

    def slot_of(block, at_chip, c):
        return 1 + (lax.rem(block - 2 * at_chip + tp, tp) - 2) * chunks + c

    def across(k, i):
        peer = lax.rem(chip + k, chips) * 2 + core
        swap, c = plan(i, core)
        owner = chip * 2 + (core + swap) % 2
        return remote(
            part(owner, c), part(owner, c), tok_send.at[0],
            tok_recv.at[slot_of(owner, lax.rem(chip + k, chips), c)], "tp", peer,
        )

    def across_part(k, begin, size, src):
        peer = lax.rem(chip + k, chips) * 2 + core
        c = plan(0, core)[1]
        at = pl.ds(pl.multiple_of(c * chunk + begin, 16), size)
        return remote(
            src.at[at, :], tok.at[me_t, at, :], tok_send.at[0],
            tok_recv.at[slot_of(me_t, lax.rem(chip + k, chips), c)], "tp", peer,
        )

    def beside(c):
        return remote(
            mine(c), part(me_t, c), pair_send.at[0], tok_recv.at[0], "tp", pair
        )

    def onward(block, c):
        return remote(
            part(block, c), part(block, c), fwd_send.at[0],
            tok_recv.at[slot_of(block, chip, c)], "tp", pair,
        )

    def whole(ref, send, recv, axis, peer):
        return remote(ref, ref, send.at[0], recv.at[0], axis, peer)

    def arrived(block, c):
        remote(
            part(block, c), part(block, c), pair_send.at[0], tok_recv.at[slot_of(block, chip, c)],
            "tp", pair,
        ).wait_recv()

    early = chunk * 3 // 128 * 16 if chunk >= 128 else chunk // 2
    for k in range(1, chips):
        across_part(k, 0, early, resid).start()
    for c in range(chunks):
        beside(c).start()

    for copy in small[:4]:
        copy.wait()
    lifted = cond[...].astype(jnp.float32)
    lifted = (lifted / (1.0 + jnp.exp(-lifted))).astype(jnp.bfloat16)
    lanes = lifted.shape[1]
    for i, m in enumerate((mshift, mscale, mgate)):
        sums = []
        for r in range(lifted.shape[0]):
            line = jnp.broadcast_to(lifted[r : r + 1, :], (16, lanes))
            sums.append(dot32(line, m[r * lanes : (r + 1) * lanes, :])[0:1])
        modsp[me_s, i : i + 1, :] = functools.reduce(jnp.add, sums)
    modsp[me_s, 3:8, :] = jnp.zeros((5, modsp.shape[2]), jnp.float32)

    next_s, next_t = lax.rem(me_s + 1, sp), lax.rem(me_t + 1, tp)

    for k in range(1, sp):
        remote(
            modsp.at[me_s], modsp.at[me_s], msp_send.at[0], msp_recv.at[0], "sp",
            lax.rem(me_s + k, sp),
        ).start()

    def all_sp():
        return whole(modsp.at[pl.ds(0, sp - 1)], msp_send, msp_recv, "sp", next_s)

    def all_tp():
        return whole(modtp.at[pl.ds(0, tp - 1)], mtp_send, mtp_recv, "tp", next_t)

    for copy in small[4:7]:
        copy.wait()
    load_k.wait()
    load_v.wait()
    normed = normed_tokens(context[...], gain_ref[...]).astype(jnp.bfloat16)
    own = ctxbuf.at[me_s]
    store_heads(own, 0, dot32(normed, wk[...]), kg[...])
    own[:, width:] = dot32(normed, wv[...]).astype(jnp.bfloat16)

    for copy in small[7:]:
        copy.wait()
    ob_ref[...] = jnp.zeros_like(ob_ref)
    ob_ref[:, :, : ob_in.shape[2]] = ob_in[...]

    def fill(h, carry):
        fill_bias(ob_ref, table, h)
        return carry

    lax.fori_loop(0, heads // 2, fill, 0)

    all_sp().wait_recv()
    summed = modsp[0]
    for s in range(1, sp):
        summed = summed + modsp[s]
    modtp[me_t] = summed

    def to_tp(k):
        return remote(
            modtp.at[me_t], modtp.at[me_t], mtp_send.at[0], mtp_recv.at[0], "tp",
            lax.rem(me_t + k, tp),
        )

    for k in range(1, tp):
        to_tp(k).start()
    load_tokens.wait()
    for k in range(1, chips):
        across_part(k, early, chunk - early, tok.at[me_t]).start()
    whole(tok.at[pair], pair_send, tok_recv, "tp", pair).wait_recv()
    for i in range(1, chunks):
        for k in range(1, chips):
            across(k, i).start()

    twin = me_s + 1 - 2 * (me_s % 2)
    steps = sp // 2

    def context_copy(block, peer):
        return remote(
            ctxbuf.at[block], ctxbuf.at[block], ctx_send.at[0], ctx_recv.at[block], "sp", peer
        )

    def fellow(m):
        return lax.rem(me_s + 2 * (m // 2 + 1 if m % 2 == 0 else steps - m // 2 - 1), sp)

    def context_arrived(block):
        context_copy(block, twin).wait_recv()

    context_copy(me_s, twin).start()
    for m in range(steps - 1):
        context_copy(me_s, fellow(m)).start()

    def pass_context(begin, end):
        for m in range(begin, end):
            context_arrived(fellow(m))
            context_copy(fellow(m), twin).start()

    lax.fori_loop(heads // 2, heads, fill, 0)

    load_o.start()
    load_q.wait()
    all_tp().wait_recv()
    piece = modtp.shape[2]
    for t in range(tp):
        mods[:, t * piece : (t + 1) * piece] = modtp[t]

    edge = REACH * GRID_W

    def project(block, c):
        values = tok[block, pl.ds(pl.multiple_of(c * chunk, chunk), chunk), :]
        normed = normed_tokens(values, gain_ref[...]) * (1.0 + mods[1:2, :]) + mods[0:1, :]
        normed = normed.astype(jnp.bfloat16)
        at = pl.multiple_of(block * count + c * chunk, chunk)
        store_heads(qbuf, at, dot32(normed, wq[...]), qg[...])
        at = pl.multiple_of(edge + block * count + c * chunk, GRID_W)
        store_heads(kvbuf, at, dot32(normed, wk[...]), kg[...])
        kvbuf[pl.ds(at, chunk), width:] = dot32(normed, wv[...]).astype(jnp.bfloat16)

    def local_step(c, carry):
        project(me_t, c)
        return carry

    lax.fori_loop(0, chunks, local_step, 0)
    near = min(2, steps - 1)
    pass_context(0, near)

    def pair_step(c, carry):
        project(pair, c)
        return carry

    lax.fori_loop(0, chunks, pair_step, 0)
    pass_context(near, steps - 1)

    ahead = (WIN_ROWS - REACH - 1) * GRID_W

    def up():
        return remote(
            kvbuf.at[pl.ds(edge, ahead), :], kvbuf.at[pl.ds(edge + tokens, ahead), :],
            halo_send.at[0], halo_recv.at[0], "sp", me_s - 1,
        )

    def down():
        return remote(
            kvbuf.at[pl.ds(tokens, edge), :], kvbuf.at[pl.ds(0, edge), :],
            halo_send.at[1], halo_recv.at[1], "sp", me_s + 1,
        )

    upper = chip < (chips + 1) // 2
    lower = jnp.logical_not(upper)

    def send_up(when):
        @pl.when(when & (me_s > 0))
        def _():
            up().start()

    def send_down(when):
        @pl.when(when & (me_s < sp - 1))
        def _():
            down().start()

    @pl.when(me_s == 0)
    def _():
        kvbuf[0:edge, :] = jnp.zeros((edge, 2 * width), jnp.bfloat16)

    kvbuf[edge + tokens + ahead :, :] = jnp.zeros((edge - ahead, 2 * width), jnp.bfloat16)

    @pl.when(me_s == sp - 1)
    def _():
        kvbuf[edge + tokens : edge + tokens + ahead, :] = jnp.zeros((ahead, 2 * width), jnp.bfloat16)

    ctx_count = ctxbuf.shape[0] * ctxbuf.shape[1]
    factor = HEAD_DIM ** (-0.5) * LOG2E
    span = edge
    blocks = rows // REACH
    half = 2 * GRID_W
    keys = 3 * span
    piece_rows = divisor(chunk_rows, 2) if REACH % 2 == 0 else 1
    piece = piece_rows * GRID_W
    per_dest = chunk_rows // piece_rows
    per_block = REACH // piece_rows
    bias_rows = 2 * WIN_ROWS - 1
    plain = list(range(bias_rows + 1))
    lead, trail, blank = bias_rows + 1, bias_rows + 2, bias_rows + 3

    def prepare(kb):
        at = pl.ds(pl.multiple_of(kb * span, span), span)
        vt[:, at] = kvbuf[at, width:].T

    def prepare_context():
        values = ctxbuf[:, :, width:].reshape(ctx_count, width)
        ctxvt[...] = values.T

    def tile_slot(line, side, first, last):
        r = line + REACH - 1 - 2 * side
        low, high = REACH - 1, REACH - 1 + WIN_ROWS
        inner = lead if r == low else trail if r == high else r if low < r < high else blank
        at_first = r if line >= REACH else blank
        at_last = r if line < 2 * REACH else blank
        if inner == at_first == at_last:
            return inner
        return inner + first * (at_first - inner) + last * (at_last - inner)

    def attend(b, first, last):
        at = pl.multiple_of(b * span, span)
        heads = width // HEAD_DIM

        def lanes_of(h, base):
            return slice(base + h * HEAD_DIM, base + (h + 1) * HEAD_DIM)

        def scores(h):
            queries = qbuf[pl.ds(at, span), lanes_of(h, 0)]
            slot = h % 2
            tops = [jnp.full((8, half), MASKED, jnp.float32) for _ in range(2)]
            for kb in range(3):
                part = dot_t(kvbuf[pl.ds(at + kb * span, span), lanes_of(h, 0)], queries)
                for i in range(REACH):
                    line = kb * REACH + i
                    for side in range(2):
                        spot = tile_slot(line, side, first, last)
                        if isinstance(spot, int) and spot == blank:
                            continue
                        cell = part[i * GRID_W : (i + 1) * GRID_W, side * half : (side + 1) * half]
                        cell = cell * factor + table[h, spot]
                        score[slot, line * GRID_W : (line + 1) * GRID_W, side * half : (side + 1) * half] = cell
                        tops[side] = jnp.maximum(tops[side], jnp.max(cell.reshape(-1, 8, half), axis=0))
            raw = jnp.full((8, 2 * half), -jnp.inf, jnp.float32)
            for c in range(ctx_count // span):
                ctx_key = ctxbuf[c * span // ctxbuf.shape[1] : (c + 1) * span // ctxbuf.shape[1], :, lanes_of(h, 0)]
                part = dot_t(ctx_key.reshape(span, HEAD_DIM), queries)
                score[slot, keys + c * span : keys + (c + 1) * span, :] = part
                raw = jnp.maximum(raw, jnp.max(part.reshape(-1, 8, 2 * half), axis=0))
            context_bias = cb[0:1, h : h + 1] * LOG2E
            top = jnp.maximum(jnp.concatenate(tops, axis=1), raw * factor + context_bias)
            return jnp.max(top, axis=0, keepdims=True), context_bias

        def finish_head(h, top, context_bias):
            slot = h % 2
            totals = []
            for side in range(2):
                cols = slice(side * half, (side + 1) * half)
                shift = jnp.broadcast_to(top[:, cols], (GRID_W, half))
                total = jnp.zeros((8, half), jnp.float32)
                for line in range(3 * REACH):
                    span_rows = slice(line * GRID_W, (line + 1) * GRID_W)
                    spot = tile_slot(line, side, first, last)
                    if isinstance(spot, int) and spot == blank:
                        prob[slot, span_rows, cols] = jnp.zeros((GRID_W, half), jnp.bfloat16)
                        continue
                    cell = jnp.exp2(score[slot, span_rows, cols] - shift)
                    total = total + jnp.sum(cell.reshape(-1, 8, half), axis=0)
                    prob[slot, span_rows, cols] = cell.astype(jnp.bfloat16)
                shift = shift - context_bias
                for c in range(ctx_count // GRID_W):
                    span_rows = slice(keys + c * GRID_W, keys + (c + 1) * GRID_W)
                    cell = jnp.exp2(score[slot, span_rows, cols] * factor - shift)
                    total = total + jnp.sum(cell.reshape(-1, 8, half), axis=0)
                    prob[slot, span_rows, cols] = cell.astype(jnp.bfloat16)
                totals.append(jnp.sum(total, axis=0, keepdims=True))
            out = dot32(vt[lanes_of(h, 0), pl.ds(at, keys)], prob[slot, :keys, :])
            out = out + dot32(ctxvt[lanes_of(h, 0), :], prob[slot, keys:, :])
            out = out * (1.0 / jnp.concatenate(totals, axis=1))
            att[pl.ds(at, span), lanes_of(h, 0)] = out.T.astype(jnp.bfloat16)

        state = scores(0)
        for h in range(heads):
            following = scores(h + 1) if h + 1 < heads else None
            finish_head(h, *state)
            state = following

    def hand(p):
        dest = p // per_dest
        local = p % per_dest
        src = pl.ds(pl.multiple_of(p * piece, piece), piece)
        dst = pl.ds(pl.multiple_of(local * piece, piece), piece)
        return remote(
            att.at[src, :], full.at[me_t, dst, :], att_send.at[0],
            att_recv.at[jnp.where(dest // 2 == chip, 0, 1 + local)], "tp", dest,
        )

    def choose(index, for_upper, for_lower):
        value = 0
        for at, (a, b) in enumerate(zip(for_upper, for_lower)):
            value = value + jnp.where(index == at, jnp.where(upper, a, b), 0)
        return value

    def wait_top():
        @pl.when(me_s > 0)
        def _():
            down().wait_recv()

    def wait_bottom():
        @pl.when(me_s < sp - 1)
        def _():
            up().wait_recv()

    def attend_block(b):
        first = jnp.where((b == 0) & (me_s == 0), 1, 0)
        last = jnp.where((b == blocks - 1) & (me_s == sp - 1), 1, 0)
        outer = first + last

        @pl.when(outer == 0)
        def _():
            attend(b, 0, 0)

        @pl.when(outer > 0)
        def _():
            attend(b, first, last)

    def hand_block(b):
        for i in range(per_block):
            p = b * per_block + per_block - 1 - i

            @pl.when(p // per_dest != me_t)
            def _():
                hand(p).start()

    def far(k, i, on_arrival=None):
        far_chip = lax.rem(chip + k, chips)
        swap, c = plan(i, core)
        block = far_chip * 2 + (core + swap) % 2
        arrived(block, c)
        onward(block, c).start()
        if on_arrival is not None:
            on_arrival()
        project(block, c)
        swap, c = plan(i, 1 - core)
        block = far_chip * 2 + (1 - core + swap) % 2
        arrived(block, c)
        project(block, c)

    def context_ready():
        context_arrived(twin)
        for m in range(1, steps):
            context_arrived(lax.rem(twin + 2 * m, sp))
        prepare_context()

    if weave:
        send_up(upper)

        def prepare_all(for_upper, for_lower):
            for a, b in zip(for_upper, for_lower):
                prepare(jnp.where(upper, a, b))

        prepare_all((1, 2, 3), (4, 5, 6))

        def attend_step(j, carry):
            b = choose(j, (1, 5, 4, 3, 2, 0), (4, 2, 1, 0, 3, 5))

            @pl.when(b == 0)
            def _():
                wait_top()
                prepare(0)

            @pl.when(b == blocks - 1)
            def _():
                wait_bottom()
                prepare(blocks + 1)

            attend_block(b)

            @pl.when(b != early_block)
            def _():
                hand_block(b)

            return carry

        early_block = jnp.where(upper, 5, 2)

        def weave_step(i, carry):
            def hand_early():
                @pl.when(i == 2)
                def _():
                    hand_block(early_block)

            far(1, i, hand_early)
            send_down((lower & (i == 0)) | (upper & (i == 1)))
            send_up(lower & (i == 2))

            @pl.when(i == 1)
            def _():
                context_ready()
                prepare_all((5, 6), (2, 3))

            @pl.when(i == 2)
            def _():
                prepare_all((4,), (1,))

            begin = jnp.where(i == 2, 2, 0)
            end = jnp.where(i == 0, 0, jnp.where(i == 2, blocks, 2))
            lax.fori_loop(begin, end, attend_step, 0)
            return carry

        lax.fori_loop(0, chunks, weave_step, 0)
    else:
        def far_step(i, carry):
            far(1 + i // chunks, lax.rem(i, chunks))
            return carry

        def prepare_step(kb, carry):
            prepare(kb)
            return carry

        def plain_step(b, carry):
            attend_block(b)
            hand_block(b)
            return carry

        lax.fori_loop(0, (chips - 1) * chunks, far_step, 0)
        send_up(me_s >= 0)
        send_down(me_s >= 0)
        context_ready()
        wait_top()
        wait_bottom()
        lax.fori_loop(0, blocks + 2, prepare_step, 0)
        lax.fori_loop(0, blocks, plain_step, 0)

    own = pl.ds(pl.multiple_of(me_t * count, count), count)
    full[me_t] = att[own, :]
    load_o.wait()

    tile = HEAD_DIM * divisor(d // HEAD_DIM, 4)

    def project_out(peer, at, lanes):
        return dot32(full[peer, at, :], wo[pl.ds(pl.multiple_of(peer * width, width), width), lanes])

    def own_column(n, carry):
        lanes = pl.ds(pl.multiple_of(n * tile, tile), tile)
        partial[:, lanes] = project_out(me_t, slice(None), lanes)
        return carry

    def pair_column(n, carry):
        lanes = pl.ds(pl.multiple_of(n * tile, tile), tile)
        partial[:, lanes] += project_out(pair, slice(None), lanes)
        return carry

    lax.fori_loop(0, d // tile, own_column, 0, unroll=True)
    whole(full.at[pair], att_send, att_recv, "tp", pair).wait_recv()
    lax.fori_loop(0, d // tile, pair_column, 0, unroll=True)

    def far_piece(step, carry):
        j = per_dest - 1 - step
        at = pl.ds(pl.multiple_of(j * piece, piece), piece)
        peers = [
            lax.rem(chip + k, chips) * 2 + side for k in range(1, chips) for side in range(2)
        ]
        landed = full.at[pl.ds(0, tp - 2), at, :]
        remote(landed, landed, att_send.at[0], att_recv.at[1 + j], "tp", pair).wait_recv()

        def column(n, inner):
            lanes = pl.ds(pl.multiple_of(n * tile, tile), tile)
            result = partial[at, lanes]
            for peer in peers:
                result = result + project_out(peer, at, lanes)
            floats = tok[me_t, at, lanes].astype(jnp.float32)
            out_ref[at, lanes] = (floats + mods[2:3, lanes] * result).astype(jnp.bfloat16)
            return inner

        lax.fori_loop(0, d // tile, column, 0, unroll=True)
        return carry

    lax.fori_loop(0, per_dest, far_piece, 0)

    whole(tok.at[pl.ds(0, 1)], pair_send, tok_recv, "tp", pair).wait_send()
    whole(tok.at[pl.ds(0, chips - 1)], tok_send, tok_recv, "tp", pair).wait_send()
    whole(tok.at[pl.ds(0, chips - 1)], fwd_send, tok_recv, "tp", pair).wait_send()
    whole(att.at[pl.ds(0, tokens - count), :], att_send, att_recv, "tp", pair).wait_send()
    whole(ctxbuf.at[pl.ds(0, sp - 1)], ctx_send, ctx_recv, "sp", next_s).wait_send()
    all_sp().wait_send()
    all_tp().wait_send()

    @pl.when(me_s > 0)
    def _():
        up().wait_send()

    @pl.when(me_s < sp - 1)
    def _():
        down().wait_send()


def shards(
    resid,
    cond,
    mod_shift,
    mod_scale,
    mod_gate,
    norm_gain,
    context,
    w_query,
    w_key,
    w_value,
    query_gain,
    key_gain,
    offset_bias,
    context_bias,
    w_out,
):
    sp, tp = lax.axis_size("sp"), lax.axis_size("tp")
    count, d = resid.shape
    width = w_query.shape[1]
    heads = width // HEAD_DIM
    tokens = count * tp
    lanes = min(cond.shape[0], HEAD_DIM)
    chunk_rows = count // GRID_W
    chunks = divisor(chunk_rows, 3)
    pieces = chunk_rows // divisor(chunk_rows, 2)
    ctx_count = context.shape[0] * sp
    span = REACH * GRID_W
    chips = tp // 2
    bf, f32 = jnp.bfloat16, jnp.float32
    piece = mod_shift.shape[1]
    vmem = pl.BlockSpec(memory_space=pltpu.VMEM)
    hbm = pl.BlockSpec(memory_space=pltpu.HBM)
    sems = pltpu.SemaphoreType.DMA
    return pl.pallas_call(
        functools.partial(layer_kernel, sp, tp, chunks),
        in_specs=[hbm] * 15,
        out_specs=vmem,
        out_shape=pltpu.VMEM((count, d), bf),
        scratch_shapes=[
            pltpu.VMEM((1, heads), f32),
            pltpu.VMEM((cond.shape[0] // lanes, lanes), bf),
            pltpu.VMEM(mod_shift.shape, bf),
            pltpu.VMEM(mod_scale.shape, bf),
            pltpu.VMEM(mod_gate.shape, bf),
            pltpu.VMEM((1, d), f32),
            pltpu.VMEM(context.shape, bf),
            pltpu.VMEM((1, HEAD_DIM), f32),
            pltpu.VMEM((1, HEAD_DIM), f32),
            pltpu.VMEM((offset_bias.shape[1], heads, offset_bias.shape[2]), f32),
            pltpu.VMEM((tp, count, d), bf),
            pltpu.VMEM((d, width), bf),
            pltpu.VMEM((d, width), bf),
            pltpu.VMEM((d, width), bf),
            pltpu.VMEM((width * tp, d), bf),
            pltpu.VMEM((tokens, width), bf),
            pltpu.VMEM((tokens + 2 * REACH * GRID_W, 2 * width), bf),
            pltpu.VMEM((sp, context.shape[0], 2 * width), bf),
            pltpu.VMEM((offset_bias.shape[1], heads, 2 * GRID_W), f32),
            pltpu.VMEM((heads, 2 * WIN_ROWS + 3, GRID_W, 2 * GRID_W), f32),
            pltpu.VMEM((sp, 8, piece), f32),
            pltpu.VMEM((tp, 8, piece), f32),
            pltpu.VMEM((8, d), f32),
            pltpu.VMEM((tokens, width), bf),
            pltpu.VMEM((tp, count, width), bf),
            pltpu.VMEM((width, tokens + 2 * span), bf),
            pltpu.VMEM((width, ctx_count), bf),
            pltpu.VMEM((2, 3 * span + ctx_count, span), f32),
            pltpu.VMEM((2, 3 * span + ctx_count, span), bf),
            pltpu.VMEM((count, d), f32),
            sems((15,)),
            sems((1,)),
            sems((1,)),
            sems((1,)),
            sems((1 + (tp - 2) * chunks,)),
            sems((1,)),
            sems((1,)),
            sems((1,)),
            sems((1,)),
            sems((1,)),
            sems((sp,)),
            sems((2,)),
            sems((2,)),
            sems((1,)),
            sems((1 + pieces,)),
        ],
        compiler_params=pltpu.CompilerParams(
            collective_id=0, has_side_effects=True, vmem_limit_bytes=VMEM_BYTES
        ),
        name="layer",
    )(
        context_bias[None, :], resid, cond.reshape(-1, lanes), mod_shift, mod_scale, mod_gate, norm_gain[None, :],
        context, w_query, w_key, w_value, query_gain[None, :], key_gain[None, :],
        jnp.transpose(offset_bias, (1, 0, 2)), w_out,
    )


def solution(mesh):
    in_specs = (
        P(("sp", "tp"), None),
        P("sp"),
        P("sp", "tp"),
        P("sp", "tp"),
        P("sp", "tp"),
        P(),
        P("sp", None),
        P(None, "tp"),
        P(None, "tp"),
        P(None, "tp"),
        P(),
        P(),
        P("tp", None, None),
        P("tp"),
        P(),
    )
    out_specs = P(("sp", "tp"), None)
    return jax.shard_map(shards, mesh=mesh, in_specs=in_specs, out_specs=out_specs, check_vma=False)
```

```python
import functools

import jax
import jax.numpy as jnp
from jax import lax
from jax.experimental import pallas as pl
from jax.experimental.pallas import tpu as pltpu
from jax.sharding import PartitionSpec as P

HEAD_DIM = 128
GRID_W = 64
WIN_ROWS = 8
WIN_COLS = 16
REACH = WIN_ROWS // 2
EPS = 1e-06
LOG2E = 1.4426950408889634
MASKED = -1e30
VMEM_BYTES = 56 * 1024 * 1024


def dot32(a, b):
    return jnp.dot(a, b, preferred_element_type=jnp.float32)


def dot_t(a, b):
    return lax.dot_general(a, b, (((1,), (1,)), ((), ())), preferred_element_type=jnp.float32)


def divisor(count, most):
    return max(d for d in range(1, most + 1) if count % d == 0)


def normed_tokens(rows, gain):
    floats = rows.astype(jnp.float32)
    inverse = lax.rsqrt(jnp.mean(floats * floats, axis=-1, keepdims=True) + EPS)
    return floats * inverse * gain


def store_heads(out_ref, at, values, gain):
    count = values.shape[0]
    for h in range(values.shape[1] // HEAD_DIM):
        part = values[:, h * HEAD_DIM : (h + 1) * HEAD_DIM]
        part = part * lax.rsqrt(jnp.mean(part * part, axis=-1, keepdims=True) + EPS) * gain
        out_ref[pl.ds(at, count), h * HEAD_DIM : (h + 1) * HEAD_DIM] = part.astype(jnp.bfloat16)


def fill_bias(ob_ref, table, h):
    rows = 2 * WIN_ROWS - 1
    lanes = 2 * GRID_W
    lane = lax.broadcasted_iota(jnp.int32, (lanes, lanes), 1)
    line = lax.broadcasted_iota(jnp.int32, (lanes, lanes), 0)
    query = line % GRID_W
    begin = jnp.clip(query - WIN_COLS // 2, 0, GRID_W - WIN_COLS)
    valid = (lane >= begin) & (lane < begin + WIN_COLS)

    def spread(r):
        row = jnp.broadcast_to(ob_ref[r, pl.ds(h, 1), :], (GRID_W, lanes))
        return pltpu.roll(row, lanes - (WIN_COLS - 1), 1, stride=1, stride_axis=0)

    masked = jnp.full((GRID_W, lanes), MASKED, jnp.float32)

    def put(slot, first, second):
        both = jnp.concatenate([first, second], axis=0) * LOG2E
        both = jnp.where(valid, both, MASKED)
        table[h, slot] = both.T[:GRID_W]

    low, high = REACH - 1, REACH - 1 + WIN_ROWS
    spreads = [spread(r) for r in range(rows)]
    for r in range(rows + 1):
        put(r, spreads[r] if r < rows else masked, spreads[r - 1] if r > 0 else masked)
    put(rows + 1, spreads[low], masked)
    put(rows + 2, masked, spreads[high - 1])
    table[h, rows + 3] = masked


def layer_kernel(
    sp, tp, chunks, cb_hbm, resid, cond_hbm, mshift_hbm, mscale_hbm, mgate_hbm, gain_hbm, context_hbm,
    wq_hbm, wk_hbm, wv_hbm, qg_hbm, kg_hbm, ob_hbm, wo_hbm, out_ref,
    cb, cond, mshift, mscale, mgate, gain_ref, context, qg, kg, ob_in,
    tok, wq, wk, wv, wo, qbuf, kvbuf, ctxbuf, ob_ref, table, modsp, modtp, mods, att, full,
    vt, ctxvt, score, prob, partial,
    load_sem, tok_send, pair_send, fwd_send, tok_recv, msp_send, msp_recv, mtp_send, mtp_recv,
    ctx_send, ctx_recv, halo_send, halo_recv, att_send, att_recv, ready, go,
):
    me_s, me_t = lax.axis_index("sp"), lax.axis_index("tp")
    count, d = resid.shape
    chunk = count // chunks
    width = wq.shape[1]
    heads = width // HEAD_DIM
    tokens = count * tp
    rows = tokens // GRID_W
    total_rows = rows * sp
    first = me_s * rows
    chips = tp // 2
    chip, core = me_t // 2, me_t % 2
    pair = chip * 2 + (1 - core)

    def remote(src, dst, send, recv, axis, peer):
        return pltpu.make_async_remote_copy(
            src_ref=src, dst_ref=dst, send_sem=send, recv_sem=recv,
            device_id={axis: peer}, device_id_type=pl.DeviceIdType.MESH,
        )

    barrier = pltpu.get_barrier_semaphore()

    def signal(semaphore, axis, peer):
        pl.semaphore_signal(
            semaphore, inc=1, device_id={axis: peer}, device_id_type=pl.DeviceIdType.MESH
        )

    for k in range(1, tp):
        other = lax.rem(me_t + k, tp)

        @pl.when(other != 0)
        def _():
            signal(barrier, "tp", other)

    def load(index, src, dst):
        return pltpu.make_async_copy(src, dst, load_sem.at[index])

    small = [
        load(i, src, dst)
        for i, (src, dst) in enumerate(
            (
                (cond_hbm, cond), (mshift_hbm, mshift), (mscale_hbm, mscale), (mgate_hbm, mgate),
                (context_hbm, context), (gain_hbm, gain_ref), (kg_hbm, kg), (qg_hbm, qg),
                (ob_hbm, ob_in), (cb_hbm, cb),
            )
        )
    ]
    base = len(small)
    load_k, load_v = load(base, wk_hbm, wk), load(base + 1, wv_hbm, wv)
    load_q, load_o = load(base + 2, wq_hbm, wq), load(base + 3, wo_hbm, wo)
    load_tokens = load(base + 4, resid, tok.at[me_t])
    for copy in small[:6] + [load_tokens, load_k, load_v] + small[6:] + [load_q]:
        copy.start()

    @pl.when(me_t != 0)
    def _():
        pl.semaphore_wait(barrier, tp - 1)
        signal(ready, "tp", 0)

    @pl.when(me_t == 0)
    def _():
        pl.semaphore_wait(ready, tp - 1)
        for k in range(1, sp):
            signal(barrier, "sp", lax.rem(me_s + k, sp))


    def part(block, c):
        return tok.at[block, pl.ds(pl.multiple_of(c * chunk, chunk), chunk), :]

    def mine(c):
        return resid.at[pl.ds(pl.multiple_of(c * chunk, chunk), chunk), :]

    chunk_rows = rows // tp
    weave = chips == 2 and chunks == 3 and chunk_rows == 6

    def plan(i, side):
        if not weave:
            return 0, i
        return jnp.where(i == 1 + side, 1, 0), jnp.where(i == 0, chunks - 1, side)

    def slot_of(block, at_chip, c):
        return 1 + (lax.rem(block - 2 * at_chip + tp, tp) - 2) * chunks + c

    def across(k, i):
        peer = lax.rem(chip + k, chips) * 2 + core
        swap, c = plan(i, core)
        owner = chip * 2 + (core + swap) % 2
        return remote(
            part(owner, c), part(owner, c), tok_send.at[0],
            tok_recv.at[slot_of(owner, lax.rem(chip + k, chips), c)], "tp", peer,
        )

    def across_part(k, begin, size, src):
        peer = lax.rem(chip + k, chips) * 2 + core
        c = plan(0, core)[1]
        at = pl.ds(pl.multiple_of(c * chunk + begin, 16), size)
        return remote(
            src.at[at, :], tok.at[me_t, at, :], tok_send.at[0],
            tok_recv.at[slot_of(me_t, lax.rem(chip + k, chips), c)], "tp", peer,
        )

    def beside(c):
        return remote(
            mine(c), part(me_t, c), pair_send.at[0], tok_recv.at[0], "tp", pair
        )

    def onward(block, c):
        return remote(
            part(block, c), part(block, c), fwd_send.at[0],
            tok_recv.at[slot_of(block, chip, c)], "tp", pair,
        )

    def whole(ref, send, recv, axis, peer):
        return remote(ref, ref, send.at[0], recv.at[0], axis, peer)

    def arrived(block, c):
        remote(
            part(block, c), part(block, c), pair_send.at[0], tok_recv.at[slot_of(block, chip, c)],
            "tp", pair,
        ).wait_recv()

    early = chunk // 64 * 48 if chunk >= 128 else chunk // 2
    for k in range(1, chips):
        across_part(k, 0, early, resid).start()
    for c in range(chunks):
        beside(c).start()

    for copy in small[:4]:
        copy.wait()
    lifted = cond[...].astype(jnp.float32)
    lifted = (lifted / (1.0 + jnp.exp(-lifted))).astype(jnp.bfloat16)
    lanes = lifted.shape[1]
    for i, m in enumerate((mshift, mscale, mgate)):
        sums = []
        for r in range(lifted.shape[0]):
            line = jnp.broadcast_to(lifted[r : r + 1, :], (16, lanes))
            sums.append(dot32(line, m[r * lanes : (r + 1) * lanes, :])[0:1])
        modsp[me_s, i : i + 1, :] = functools.reduce(jnp.add, sums)
    modsp[me_s, 3:8, :] = jnp.zeros((5, modsp.shape[2]), jnp.float32)

    next_s, next_t = lax.rem(me_s + 1, sp), lax.rem(me_t + 1, tp)

    def all_sp():
        return whole(modsp.at[pl.ds(0, sp - 1)], msp_send, msp_recv, "sp", next_s)

    def all_tp():
        return whole(modtp.at[pl.ds(0, tp - 1)], mtp_send, mtp_recv, "tp", next_t)

    for copy in small[4:7]:
        copy.wait()
    load_k.wait()
    load_v.wait()
    normed = normed_tokens(context[...], gain_ref[...]).astype(jnp.bfloat16)
    own = ctxbuf.at[me_s]
    store_heads(own, 0, dot32(normed, wk[...]), kg[...])
    own[:, width:] = dot32(normed, wv[...]).astype(jnp.bfloat16)

    @pl.when(me_t == 0)
    def _():
        pl.semaphore_wait(barrier, sp - 1)
        for k in range(1, tp):
            signal(go, "tp", k)

    @pl.when(me_t != 0)
    def _():
        pl.semaphore_wait(go, 1)

    for k in range(1, sp):
        remote(
            modsp.at[me_s], modsp.at[me_s], msp_send.at[0], msp_recv.at[0], "sp",
            lax.rem(me_s + k, sp),
        ).start()

    for copy in small[7:]:
        copy.wait()
    ob_ref[...] = jnp.zeros_like(ob_ref)
    ob_ref[:, :, : ob_in.shape[2]] = ob_in[...]

    def fill(h, carry):
        fill_bias(ob_ref, table, h)
        return carry

    lax.fori_loop(0, heads // 2, fill, 0)

    all_sp().wait_recv()
    summed = modsp[0]
    for s in range(1, sp):
        summed = summed + modsp[s]
    modtp[me_t] = summed

    def to_tp(k):
        return remote(
            modtp.at[me_t], modtp.at[me_t], mtp_send.at[0], mtp_recv.at[0], "tp",
            lax.rem(me_t + k, tp),
        )

    for k in range(1, tp):
        to_tp(k).start()
    load_tokens.wait()
    for k in range(1, chips):
        across_part(k, early, chunk - early, tok.at[me_t]).start()
    whole(tok.at[pair], pair_send, tok_recv, "tp", pair).wait_recv()
    for i in range(1, chunks):
        for k in range(1, chips):
            across(k, i).start()

    twin = me_s + 1 - 2 * (me_s % 2)
    steps = sp // 2

    def context_copy(block, peer):
        return remote(
            ctxbuf.at[block], ctxbuf.at[block], ctx_send.at[0], ctx_recv.at[block], "sp", peer
        )

    def fellow(m):
        return lax.rem(me_s + 2 * (m // 2 + 1 if m % 2 == 0 else steps - m // 2 - 1), sp)

    def context_arrived(block):
        context_copy(block, twin).wait_recv()

    context_copy(me_s, twin).start()
    for m in range(steps - 1):
        context_copy(me_s, fellow(m)).start()

    def pass_context(begin, end):
        for m in range(begin, end):
            context_arrived(fellow(m))
            context_copy(fellow(m), twin).start()

    lax.fori_loop(heads // 2, heads, fill, 0)

    load_o.start()
    load_q.wait()
    all_tp().wait_recv()
    piece = modtp.shape[2]
    for t in range(tp):
        mods[:, t * piece : (t + 1) * piece] = modtp[t]

    edge = REACH * GRID_W

    def project(block, c):
        values = tok[block, pl.ds(pl.multiple_of(c * chunk, chunk), chunk), :]
        normed = normed_tokens(values, gain_ref[...]) * (1.0 + mods[1:2, :]) + mods[0:1, :]
        normed = normed.astype(jnp.bfloat16)
        at = pl.multiple_of(block * count + c * chunk, chunk)
        store_heads(qbuf, at, dot32(normed, wq[...]), qg[...])
        at = pl.multiple_of(edge + block * count + c * chunk, GRID_W)
        store_heads(kvbuf, at, dot32(normed, wk[...]), kg[...])
        kvbuf[pl.ds(at, chunk), width:] = dot32(normed, wv[...]).astype(jnp.bfloat16)

    def local_step(c, carry):
        project(me_t, c)
        return carry

    lax.fori_loop(0, chunks, local_step, 0)
    near = min(2, steps - 1)
    pass_context(0, near)

    def pair_step(c, carry):
        project(pair, c)
        return carry

    lax.fori_loop(0, chunks, pair_step, 0)
    pass_context(near, steps - 1)

    ahead = (WIN_ROWS - REACH - 1) * GRID_W

    def up():
        return remote(
            kvbuf.at[pl.ds(edge, ahead), :], kvbuf.at[pl.ds(edge + tokens, ahead), :],
            halo_send.at[0], halo_recv.at[0], "sp", me_s - 1,
        )

    def down():
        return remote(
            kvbuf.at[pl.ds(tokens, edge), :], kvbuf.at[pl.ds(0, edge), :],
            halo_send.at[1], halo_recv.at[1], "sp", me_s + 1,
        )

    upper = chip < (chips + 1) // 2
    lower = jnp.logical_not(upper)

    def send_up(when):
        @pl.when(when & (me_s > 0))
        def _():
            up().start()

    def send_down(when):
        @pl.when(when & (me_s < sp - 1))
        def _():
            down().start()

    @pl.when(me_s == 0)
    def _():
        kvbuf[0:edge, :] = jnp.zeros((edge, 2 * width), jnp.bfloat16)

    kvbuf[edge + tokens + ahead :, :] = jnp.zeros((edge - ahead, 2 * width), jnp.bfloat16)

    @pl.when(me_s == sp - 1)
    def _():
        kvbuf[edge + tokens : edge + tokens + ahead, :] = jnp.zeros((ahead, 2 * width), jnp.bfloat16)

    ctx_count = ctxbuf.shape[0] * ctxbuf.shape[1]
    factor = HEAD_DIM ** (-0.5) * LOG2E
    span = edge
    blocks = rows // REACH
    half = 2 * GRID_W
    keys = 3 * span
    piece_rows = divisor(chunk_rows, 2) if REACH % 2 == 0 else 1
    piece = piece_rows * GRID_W
    per_dest = chunk_rows // piece_rows
    per_block = REACH // piece_rows
    bias_rows = 2 * WIN_ROWS - 1
    plain = list(range(bias_rows + 1))
    lead, trail, blank = bias_rows + 1, bias_rows + 2, bias_rows + 3

    def prepare(kb):
        at = pl.ds(pl.multiple_of(kb * span, span), span)
        vt[:, at] = kvbuf[at, width:].T

    def prepare_context():
        values = ctxbuf[:, :, width:].reshape(ctx_count, width)
        ctxvt[...] = values.T

    def tile_slot(line, side, first, last):
        r = line + REACH - 1 - 2 * side
        low, high = REACH - 1, REACH - 1 + WIN_ROWS
        inner = lead if r == low else trail if r == high else r if low < r < high else blank
        at_first = r if line >= REACH else blank
        at_last = r if line < 2 * REACH else blank
        if inner == at_first == at_last:
            return inner
        return inner + first * (at_first - inner) + last * (at_last - inner)

    def attend(b, first, last):
        at = pl.multiple_of(b * span, span)
        heads = width // HEAD_DIM

        def lanes_of(h, base):
            return slice(base + h * HEAD_DIM, base + (h + 1) * HEAD_DIM)

        def scores(h):
            queries = qbuf[pl.ds(at, span), lanes_of(h, 0)]
            slot = h % 2
            tops = [jnp.full((8, half), MASKED, jnp.float32) for _ in range(2)]
            for kb in range(3):
                part = dot_t(kvbuf[pl.ds(at + kb * span, span), lanes_of(h, 0)], queries)
                for i in range(REACH):
                    line = kb * REACH + i
                    for side in range(2):
                        spot = tile_slot(line, side, first, last)
                        if isinstance(spot, int) and spot == blank:
                            continue
                        cell = part[i * GRID_W : (i + 1) * GRID_W, side * half : (side + 1) * half]
                        cell = cell * factor + table[h, spot]
                        score[slot, line * GRID_W : (line + 1) * GRID_W, side * half : (side + 1) * half] = cell
                        tops[side] = jnp.maximum(tops[side], jnp.max(cell.reshape(-1, 8, half), axis=0))
            raw = jnp.full((8, 2 * half), -jnp.inf, jnp.float32)
            for c in range(ctx_count // span):
                ctx_key = ctxbuf[c * span // ctxbuf.shape[1] : (c + 1) * span // ctxbuf.shape[1], :, lanes_of(h, 0)]
                part = dot_t(ctx_key.reshape(span, HEAD_DIM), queries)
                score[slot, keys + c * span : keys + (c + 1) * span, :] = part
                raw = jnp.maximum(raw, jnp.max(part.reshape(-1, 8, 2 * half), axis=0))
            context_bias = cb[0:1, h : h + 1] * LOG2E
            top = jnp.maximum(jnp.concatenate(tops, axis=1), raw * factor + context_bias)
            return jnp.max(top, axis=0, keepdims=True), context_bias

        def finish_head(h, top, context_bias):
            slot = h % 2
            totals = []
            for side in range(2):
                cols = slice(side * half, (side + 1) * half)
                shift = jnp.broadcast_to(top[:, cols], (GRID_W, half))
                total = jnp.zeros((8, half), jnp.float32)
                for line in range(3 * REACH):
                    span_rows = slice(line * GRID_W, (line + 1) * GRID_W)
                    spot = tile_slot(line, side, first, last)
                    if isinstance(spot, int) and spot == blank:
                        prob[slot, span_rows, cols] = jnp.zeros((GRID_W, half), jnp.bfloat16)
                        continue
                    cell = jnp.exp2(score[slot, span_rows, cols] - shift)
                    total = total + jnp.sum(cell.reshape(-1, 8, half), axis=0)
                    prob[slot, span_rows, cols] = cell.astype(jnp.bfloat16)
                shift = shift - context_bias
                for c in range(ctx_count // GRID_W):
                    span_rows = slice(keys + c * GRID_W, keys + (c + 1) * GRID_W)
                    cell = jnp.exp2(score[slot, span_rows, cols] * factor - shift)
                    total = total + jnp.sum(cell.reshape(-1, 8, half), axis=0)
                    prob[slot, span_rows, cols] = cell.astype(jnp.bfloat16)
                totals.append(jnp.sum(total, axis=0, keepdims=True))
            out = dot32(vt[lanes_of(h, 0), pl.ds(at, keys)], prob[slot, :keys, :])
            out = out + dot32(ctxvt[lanes_of(h, 0), :], prob[slot, keys:, :])
            out = out * (1.0 / jnp.concatenate(totals, axis=1))
            att[pl.ds(at, span), lanes_of(h, 0)] = out.T.astype(jnp.bfloat16)

        state = scores(0)
        for h in range(heads):
            following = scores(h + 1) if h + 1 < heads else None
            finish_head(h, *state)
            state = following

    def hand(p):
        dest = p // per_dest
        local = p % per_dest
        src = pl.ds(pl.multiple_of(p * piece, piece), piece)
        dst = pl.ds(pl.multiple_of(local * piece, piece), piece)
        return remote(
            att.at[src, :], full.at[me_t, dst, :], att_send.at[0],
            att_recv.at[jnp.where(dest // 2 == chip, 0, 1 + local)], "tp", dest,
        )

    def choose(index, for_upper, for_lower):
        value = 0
        for at, (a, b) in enumerate(zip(for_upper, for_lower)):
            value = value + jnp.where(index == at, jnp.where(upper, a, b), 0)
        return value

    def wait_top():
        @pl.when(me_s > 0)
        def _():
            down().wait_recv()

    def wait_bottom():
        @pl.when(me_s < sp - 1)
        def _():
            up().wait_recv()

    def attend_block(b):
        first = jnp.where((b == 0) & (me_s == 0), 1, 0)
        last = jnp.where((b == blocks - 1) & (me_s == sp - 1), 1, 0)
        outer = first + last

        @pl.when(outer == 0)
        def _():
            attend(b, 0, 0)

        @pl.when(outer > 0)
        def _():
            attend(b, first, last)

    def hand_block(b):
        for i in range(per_block):
            p = b * per_block + per_block - 1 - i

            @pl.when(p // per_dest != me_t)
            def _():
                hand(p).start()

    def far(k, i, on_arrival=None):
        far_chip = lax.rem(chip + k, chips)
        swap, c = plan(i, core)
        block = far_chip * 2 + (core + swap) % 2
        arrived(block, c)
        onward(block, c).start()
        if on_arrival is not None:
            on_arrival()
        project(block, c)
        swap, c = plan(i, 1 - core)
        block = far_chip * 2 + (1 - core + swap) % 2
        arrived(block, c)
        project(block, c)

    def context_ready():
        context_arrived(twin)
        for m in range(1, steps):
            context_arrived(lax.rem(twin + 2 * m, sp))
        prepare_context()

    if weave:
        send_up(upper)

        def prepare_all(for_upper, for_lower):
            for a, b in zip(for_upper, for_lower):
                prepare(jnp.where(upper, a, b))

        prepare_all((1, 2, 3), (4, 5, 6))

        def attend_step(j, carry):
            b = choose(j, (1, 5, 4, 3, 2, 0), (4, 2, 1, 0, 3, 5))

            @pl.when(b == 0)
            def _():
                wait_top()
                prepare(0)

            @pl.when(b == blocks - 1)
            def _():
                wait_bottom()
                send_down(upper)
                prepare(blocks + 1)

            attend_block(b)

            @pl.when(b != early_block)
            def _():
                hand_block(b)

            return carry

        early_block = jnp.where(upper, 5, 2)

        def weave_step(i, carry):
            def hand_early():
                @pl.when(i == 2)
                def _():
                    hand_block(early_block)

            far(1, i, hand_early)
            send_down(lower & (i == 0))
            send_up(lower & (i == 2))

            @pl.when(i == 1)
            def _():
                context_ready()
                prepare_all((5, 6), (2, 3))

            @pl.when(i == 2)
            def _():
                prepare_all((4,), (1,))

            begin = jnp.where(i == 2, 2, 0)
            end = jnp.where(i == 0, 0, jnp.where(i == 2, blocks, 2))
            lax.fori_loop(begin, end, attend_step, 0)
            return carry

        lax.fori_loop(0, chunks, weave_step, 0)
    else:
        def far_step(i, carry):
            far(1 + i // chunks, lax.rem(i, chunks))
            return carry

        def prepare_step(kb, carry):
            prepare(kb)
            return carry

        def plain_step(b, carry):
            attend_block(b)
            hand_block(b)
            return carry

        lax.fori_loop(0, (chips - 1) * chunks, far_step, 0)
        send_up(me_s >= 0)
        send_down(me_s >= 0)
        context_ready()
        wait_top()
        wait_bottom()
        lax.fori_loop(0, blocks + 2, prepare_step, 0)
        lax.fori_loop(0, blocks, plain_step, 0)

    own = pl.ds(pl.multiple_of(me_t * count, count), count)
    full[me_t] = att[own, :]
    load_o.wait()

    tile = HEAD_DIM * divisor(d // HEAD_DIM, 4)

    def project_out(peer, at, lanes):
        return dot32(full[peer, at, :], wo[pl.ds(pl.multiple_of(peer * width, width), width), lanes])

    def own_column(n, carry):
        lanes = pl.ds(pl.multiple_of(n * tile, tile), tile)
        partial[:, lanes] = project_out(me_t, slice(None), lanes)
        return carry

    def pair_column(n, carry):
        lanes = pl.ds(pl.multiple_of(n * tile, tile), tile)
        partial[:, lanes] += project_out(pair, slice(None), lanes)
        return carry

    lax.fori_loop(0, d // tile, own_column, 0, unroll=True)
    whole(full.at[pair], att_send, att_recv, "tp", pair).wait_recv()
    lax.fori_loop(0, d // tile, pair_column, 0, unroll=True)

    def far_piece(step, carry):
        j = per_dest - 1 - step
        at = pl.ds(pl.multiple_of(j * piece, piece), piece)
        peers = [
            lax.rem(chip + k, chips) * 2 + side for k in range(1, chips) for side in range(2)
        ]
        landed = full.at[pl.ds(0, tp - 2), at, :]
        remote(landed, landed, att_send.at[0], att_recv.at[1 + j], "tp", pair).wait_recv()

        def column(n, inner):
            lanes = pl.ds(pl.multiple_of(n * tile, tile), tile)
            result = partial[at, lanes]
            for peer in peers:
                result = result + project_out(peer, at, lanes)
            floats = tok[me_t, at, lanes].astype(jnp.float32)
            out_ref[at, lanes] = (floats + mods[2:3, lanes] * result).astype(jnp.bfloat16)
            return inner

        lax.fori_loop(0, d // tile, column, 0, unroll=True)
        return carry

    lax.fori_loop(0, per_dest, far_piece, 0)

    whole(tok.at[pl.ds(0, 1)], pair_send, tok_recv, "tp", pair).wait_send()
    whole(tok.at[pl.ds(0, chips - 1)], tok_send, tok_recv, "tp", pair).wait_send()
    whole(tok.at[pl.ds(0, chips - 1)], fwd_send, tok_recv, "tp", pair).wait_send()
    whole(att.at[pl.ds(0, tokens - count), :], att_send, att_recv, "tp", pair).wait_send()
    whole(ctxbuf.at[pl.ds(0, sp - 1)], ctx_send, ctx_recv, "sp", next_s).wait_send()
    all_sp().wait_send()
    all_tp().wait_send()

    @pl.when(me_s > 0)
    def _():
        up().wait_send()

    @pl.when(me_s < sp - 1)
    def _():
        down().wait_send()


def shards(
    resid,
    cond,
    mod_shift,
    mod_scale,
    mod_gate,
    norm_gain,
    context,
    w_query,
    w_key,
    w_value,
    query_gain,
    key_gain,
    offset_bias,
    context_bias,
    w_out,
):
    sp, tp = lax.axis_size("sp"), lax.axis_size("tp")
    count, d = resid.shape
    width = w_query.shape[1]
    heads = width // HEAD_DIM
    tokens = count * tp
    lanes = min(cond.shape[0], HEAD_DIM)
    chunk_rows = count // GRID_W
    chunks = divisor(chunk_rows, 3)
    pieces = chunk_rows // divisor(chunk_rows, 2)
    ctx_count = context.shape[0] * sp
    span = REACH * GRID_W
    chips = tp // 2
    bf, f32 = jnp.bfloat16, jnp.float32
    piece = mod_shift.shape[1]
    vmem = pl.BlockSpec(memory_space=pltpu.VMEM)
    hbm = pl.BlockSpec(memory_space=pltpu.HBM)
    sems = pltpu.SemaphoreType.DMA
    return pl.pallas_call(
        functools.partial(layer_kernel, sp, tp, chunks),
        in_specs=[hbm] * 15,
        out_specs=vmem,
        out_shape=pltpu.VMEM((count, d), bf),
        scratch_shapes=[
            pltpu.VMEM((1, heads), f32),
            pltpu.VMEM((cond.shape[0] // lanes, lanes), bf),
            pltpu.VMEM(mod_shift.shape, bf),
            pltpu.VMEM(mod_scale.shape, bf),
            pltpu.VMEM(mod_gate.shape, bf),
            pltpu.VMEM((1, d), f32),
            pltpu.VMEM(context.shape, bf),
            pltpu.VMEM((1, HEAD_DIM), f32),
            pltpu.VMEM((1, HEAD_DIM), f32),
            pltpu.VMEM((offset_bias.shape[1], heads, offset_bias.shape[2]), f32),
            pltpu.VMEM((tp, count, d), bf),
            pltpu.VMEM((d, width), bf),
            pltpu.VMEM((d, width), bf),
            pltpu.VMEM((d, width), bf),
            pltpu.VMEM((width * tp, d), bf),
            pltpu.VMEM((tokens, width), bf),
            pltpu.VMEM((tokens + 2 * REACH * GRID_W, 2 * width), bf),
            pltpu.VMEM((sp, context.shape[0], 2 * width), bf),
            pltpu.VMEM((offset_bias.shape[1], heads, 2 * GRID_W), f32),
            pltpu.VMEM((heads, 2 * WIN_ROWS + 3, GRID_W, 2 * GRID_W), f32),
            pltpu.VMEM((sp, 8, piece), f32),
            pltpu.VMEM((tp, 8, piece), f32),
            pltpu.VMEM((8, d), f32),
            pltpu.VMEM((tokens, width), bf),
            pltpu.VMEM((tp, count, width), bf),
            pltpu.VMEM((width, tokens + 2 * span), bf),
            pltpu.VMEM((width, ctx_count), bf),
            pltpu.VMEM((2, 3 * span + ctx_count, span), f32),
            pltpu.VMEM((2, 3 * span + ctx_count, span), bf),
            pltpu.VMEM((count, d), f32),
            sems((15,)),
            sems((1,)),
            sems((1,)),
            sems((1,)),
            sems((1 + (tp - 2) * chunks,)),
            sems((1,)),
            sems((1,)),
            sems((1,)),
            sems((1,)),
            sems((1,)),
            sems((sp,)),
            sems((2,)),
            sems((2,)),
            sems((1,)),
            sems((1 + pieces,)),
            pltpu.SemaphoreType.REGULAR,
            pltpu.SemaphoreType.REGULAR,
        ],
        compiler_params=pltpu.CompilerParams(
            collective_id=0, has_side_effects=True, vmem_limit_bytes=VMEM_BYTES
        ),
        name="layer",
    )(
        context_bias[None, :], resid, cond.reshape(-1, lanes), mod_shift, mod_scale, mod_gate, norm_gain[None, :],
        context, w_query, w_key, w_value, query_gain[None, :], key_gain[None, :],
        jnp.transpose(offset_bias, (1, 0, 2)), w_out,
    )


def solution(mesh):
    in_specs = (
        P(("sp", "tp"), None),
        P("sp"),
        P("sp", "tp"),
        P("sp", "tp"),
        P("sp", "tp"),
        P(),
        P("sp", None),
        P(None, "tp"),
        P(None, "tp"),
        P(None, "tp"),
        P(),
        P(),
        P("tp", None, None),
        P("tp"),
        P(),
    )
    out_specs = P(("sp", "tp"), None)
    return jax.shard_map(shards, mesh=mesh, in_specs=in_specs, out_specs=out_specs, check_vma=False)
```
